512 devices in a mesh: sp: 64 (over z, y), tp: 8 (over x, core).
Axes of the slice: x: 4, y: 8, z: 8, core: 2. Of those that a mesh axis runs over, the one named last changes fastest.
Arguments:
- tokens: bfloat16 [65536, 2048], P('sp'), may hold values from -6 to 6
- norm_gain: float32 [2048], replicated, may hold values from 0.1 to 1.9
- w_query: bfloat16 [2048, 512], P(None, 'tp'), may hold values from -0.79549513 to 0.79549513
- w_key: bfloat16 [2048, 128], P('sp'), may hold values from -0.79549513 to 0.79549513
- w_value: bfloat16 [2048, 128], P('sp'), may hold values from -0.125 to 0.125
- w_pool_in: bfloat16 [2048, 512], P(None, 'tp'), may hold values from -0.125 to 0.125
- sink_logit: float32 [8], P('tp'), may hold values from 3 to 7
- pool_scale: float32 [512], P('tp'), may hold values from 0.05 to 0.5
- w_out: bfloat16 [1024, 2048], P('tp', 'sp'), may hold values from -0.75 to 0.75
Outputs:
- mixed_out: bfloat16 [65536, 2048], P(('sp', 'tp'))
The draws below stay inside these ranges and needn't reach their ends.
All inputs are finite; a program needn't handle non-finite values.
Results may differ from the reference program's by a relative error of at most 0.03.
The reference program's roundings to bfloat16 on the way (of `normed`, `query`, `key`, `value`, `pool_in`, `weights`, `attended` and `pooled`) count: a program that leaves them out, or rounds other values in their place, can miss the bound.
Values may be sent and summed in bfloat16 or wider, within the bound.
A program may use at most 64 MiB of HBM per device.

```python
import math
import jax
import jax.numpy as jnp
from jax import lax

D = 2048
HEAD = 64
QH = 8
KVH = 2
POOL_CH = 128
POOL_W = 512
WINDOW = 128
QB = 128
SEQ = 65536


def projection_draw(key, shape):
    values = jax.random.truncated_normal(key, -6.0, 6.0, shape, jnp.float32) * D ** (-0.5)
    return values.astype(jnp.bfloat16)


def draw_w_query(key, part):
    return projection_draw(jax.random.fold_in(key, 11), (D, QH * HEAD))


def draw_w_key(key, part):
    return projection_draw(jax.random.fold_in(key, 23), (D, KVH * HEAD))


def level_of(key, dims, pieces, smallest, top_value):
    level = 1.0
    for dim, parts in pieces:
        steps = jax.random.uniform(jax.random.fold_in(jax.random.fold_in(key, 6), dim), (parts,), jnp.float32, smallest / len(pieces), top_value / len(pieces))
        level = level * jnp.repeat(jnp.exp(steps), dims[dim] // parts).reshape((-1,) + (1,) * (len(dims) - 1 - dim))
    return level


def centred(rng, dims, scale, reach, pieces=(), kind=jnp.bfloat16):
    entries = scale * jax.random.normal(rng, dims, jnp.float32)
    if pieces:
        entries = entries * level_of(rng, dims, pieces, -0.22, 0.18)
    return jnp.clip(entries, -reach, reach).astype(kind)


def setup_inputs(seed: int = 0) -> dict:
    seeds = jax.random.split(jax.random.key(seed), 10)
    tokens = centred(seeds[0], (SEQ, D), 1.0, 6.0, ((0, 64),))
    norm_gain = jnp.clip(1.0 + 0.18 * jax.random.normal(seeds[1], (D,), jnp.float32), 0.1, 1.9)
    w_query = draw_w_query(jax.random.fold_in(seeds[9], 71), 0)
    w_key = draw_w_key(jax.random.fold_in(seeds[9], 71), 0)
    w_value = centred(seeds[4], (D, KVH * HEAD), D ** -0.5, 0.125, ((0, 64),))
    w_pool_in = centred(seeds[5], (D, POOL_W), D ** -0.5, 0.125, ((1, 8),))
    sink_logit = jnp.clip(3.0 + 4.0 * jax.random.uniform(seeds[6], (QH,), jnp.float32) ** level_of(seeds[6], (QH,), ((0, 8),), -0.2, 0.2), 3.0, 7.0)
    pool_scale = jnp.clip(jnp.exp(math.log(0.5) - 2.3025851 * jax.random.uniform(seeds[7], (POOL_W,), jnp.float32) ** level_of(seeds[7], (POOL_W,), ((0, 8),), -0.2, 0.2)), 0.05, 0.5)
    w_out = centred(seeds[8], (QH * HEAD + POOL_W, D), (4.0 * (QH * HEAD + POOL_W) ** -0.5), 0.75, ((0, 8), (1, 64)))
    return {"tokens": tokens, "norm_gain": norm_gain, "w_query": w_query, "w_key": w_key, "w_value": w_value, "w_pool_in": w_pool_in, "sink_logit": sink_logit, "pool_scale": pool_scale, "w_out": w_out}


NEG_BIG = -1e+30
POOL_SPANS = (2, 4, 8, 16)

def layer_normed(tokens, norm_gain):
    values = tokens.astype(jnp.float32)
    center = lax.optimization_barrier(jnp.mean(values, axis=-1, keepdims=True))
    spread = lax.optimization_barrier(jnp.mean(jnp.square(values - center), axis=-1, keepdims=True))
    return ((values - center) * lax.rsqrt(spread + 1e-06) * norm_gain).astype(jnp.bfloat16)

def rotate(values, positions):
    half = HEAD // 2
    inverse = 10000.0 ** (-jnp.arange(half, dtype=jnp.float32) / half)
    angles = positions[:, None] * inverse[None, :]
    cosine = jnp.cos(angles)[:, None, :]
    sine = jnp.sin(angles)[:, None, :]
    first = values[..., :half]
    second = values[..., half:]
    return jnp.concatenate([first * cosine - second * sine, first * sine + second * cosine], axis=-1)

def reference(tokens, norm_gain, w_query, w_key, w_value, w_pool_in, sink_logit, pool_scale, w_out):
    length = tokens.shape[0]
    group = QH // KVH
    normed = layer_normed(tokens, norm_gain)
    positions = jnp.arange(length).astype(jnp.float32)
    query = rotate(jnp.dot(normed, w_query, preferred_element_type=jnp.float32).reshape(length, QH, HEAD), positions).astype(jnp.bfloat16)
    key = rotate(jnp.dot(normed, w_key, preferred_element_type=jnp.float32).reshape(length, KVH, HEAD), positions).astype(jnp.bfloat16)
    value = jnp.dot(normed, w_value, preferred_element_type=jnp.float32).astype(jnp.bfloat16).reshape(length, KVH, HEAD)
    pool_in = jnp.dot(normed, w_pool_in, preferred_element_type=jnp.float32).astype(jnp.bfloat16)
    key_padded = jnp.pad(key, ((WINDOW, WINDOW), (0, 0), (0, 0)))
    value_padded = jnp.pad(value, ((WINDOW, WINDOW), (0, 0), (0, 0)))
    span = QB + 2 * WINDOW
    sink_grid = sink_logit.reshape(KVH, group)[:, :, None, None]

    def attend(start):
        queries = lax.dynamic_slice_in_dim(query, start, QB, 0).reshape(QB, KVH, group, HEAD)
        keys = lax.dynamic_slice_in_dim(key_padded, start, span, 0)
        values = lax.dynamic_slice_in_dim(value_padded, start, span, 0)
        scores = jnp.einsum('ikgd,jkd->kgij', queries.astype(jnp.float32), keys.astype(jnp.float32)) * HEAD ** (-0.5)
        query_pos = start + jnp.arange(QB).astype(jnp.int32)
        key_pos = start - WINDOW + jnp.arange(span).astype(jnp.int32)
        valid = (jnp.abs(query_pos[:, None] - key_pos[None, :]) <= WINDOW) & (key_pos[None, :] >= 0) & (key_pos[None, :] < length)
        scores = jnp.where(valid, scores, NEG_BIG)
        highest = jnp.maximum(lax.optimization_barrier(jnp.max(scores, axis=-1, keepdims=True)), sink_grid)
        expo = jnp.where(valid, jnp.exp(scores - highest), 0.0)
        total = lax.optimization_barrier(jnp.sum(expo, axis=-1, keepdims=True)) + jnp.exp(sink_grid - highest)
        weights = (expo / total).astype(jnp.bfloat16)
        result = jnp.einsum('kgij,jkd->ikgd', weights.astype(jnp.float32), values.astype(jnp.float32))
        return result.reshape(QB, QH * HEAD).astype(jnp.bfloat16)
    starts = (jnp.arange(length // QB) * QB).astype(jnp.int32)
    attended = lax.map(attend, starts).reshape(length, QH * HEAD)
    pool_vals = pool_in.astype(jnp.float32)
    running = jnp.pad(jnp.cumsum(pool_vals, axis=0), ((1, 0), (0, 0)))
    where_at = jnp.arange(length).astype(jnp.int32)
    means = []
    for index, width in enumerate(POOL_SPANS):
        lower = jnp.clip(where_at - width // 2, 0, length)
        upper = jnp.clip(where_at + width // 2, 0, length)
        block = running[:, index * POOL_CH:(index + 1) * POOL_CH]
        means.append((block[upper] - block[lower]) / (upper - lower).astype(jnp.float32)[:, None])
    pooled = ((jnp.concatenate(means, axis=1) - pool_vals) * pool_scale).astype(jnp.bfloat16)
    joined = jnp.concatenate([attended, pooled], axis=1)
    return jnp.dot(joined, w_out, preferred_element_type=jnp.float32).astype(jnp.bfloat16)
```

```python
import functools

import jax
import jax.numpy as jnp
import numpy as np
from jax import lax
from jax.experimental import pallas as pl
from jax.experimental.pallas import tpu as pltpu
from jax.sharding import PartitionSpec as P

HEAD = 64
WINDOW = 128
QB = 128
NEG_BIG = -1e30
EDGE = 16
RING = 8
ORDER = (1, 7, 2, 6, 3, 5, 4)
MESH = pl.DeviceIdType.MESH
F32 = jnp.float32
BF16 = jnp.bfloat16


def angle_tables(n_sp, rows):
    half = HEAD // 2
    inverse = 10000.0 ** (-np.arange(half, dtype=np.float64) / half)

    def pair(positions):
        angles = positions[:, None].astype(np.float64) * inverse[None, :]
        cosine, sine = np.cos(angles), np.sin(angles)
        ones = np.ones((len(positions), HEAD))
        c = np.concatenate([cosine, cosine, ones], axis=1)
        s = np.concatenate([-sine, sine, 0.0 * ones], axis=1)
        return c.astype(np.float32), s.astype(np.float32)

    c, s = pair(np.arange(n_sp) * rows)
    start = np.zeros((n_sp, 8, 2 * HEAD), np.float32)
    start[:, 0], start[:, 1] = c, s
    return start, np.stack(pair(np.arange(rows)))


def kernel(
    rows,
    tokens,
    gain,
    w_query,
    w_key,
    w_value,
    w_pool,
    small,
    w_out,
    start_angles,
    row_angles,
    out,
    tok,
    gain_v,
    wq_v,
    wp_v,
    wk_v,
    wv_v,
    wo_v,
    small_v,
    start_v,
    angles_v,
    wqp,
    kvbuf,
    wkv,
    wbuf,
    q_v,
    p_ext,
    pool_v,
    kv_ext,
    mix_send,
    mix_recv,
    load_sem,
    tok_sem,
    kv1_s,
    kv1_r,
    kv2_s,
    kv2_r,
    kvd_s,
    kvd_r,
    w1_s,
    w1_r,
    w2_s,
    w2_r,
    w3_s,
    w3_r,
    wd_s,
    wd_r,
    ph_s,
    ph_r,
    kh_s,
    kh_r,
    mx_s,
    mx_r,
):
    s = lax.axis_index("sp")
    t = lax.axis_index("tp")
    n_sp = lax.axis_size("sp")
    n_tp = lax.axis_size("tp")
    x, c = t // 2, t % 2
    z, y = s // RING, s % RING
    a = y + c * (z - y)
    b = z + c * (y - z)
    step_a = 1 + (RING - 1) * c
    step_b = RING - (RING - 1) * c
    other = t + 1 - 2 * c

    def along_a(k):
        return (s + ((a + k) % RING - a) * step_a, t)

    def along_b(k):
        return (s + ((b + k) % RING - b) * step_b, t)

    def along_x(k):
        return (s, ((x + k) % 4) * 2 + c)

    def along_tp(k):
        return (s, (t + k) % n_tp)

    after = ((s + 1) % n_sp, t)
    before = ((s + n_sp - 1) % n_sp, t)

    barrier = pltpu.get_barrier_semaphore()
    peers = (
        [along_a(k) for k in range(1, RING)]
        + [along_b(k) for k in range(1, RING)]
        + [along_tp(k) for k in range(1, n_tp)]
        + [after, before]
    )
    for peer in peers:
        pl.semaphore_signal(barrier, inc=1, device_id=peer, device_id_type=MESH)

    def remote(src, dst, ssem, rsem, device):
        return pltpu.make_async_remote_copy(
            src_ref=src, dst_ref=dst, send_sem=ssem, recv_sem=rsem,
            device_id=device, device_id_type=MESH,
        )

    loads = [
        pltpu.make_async_copy(src, dst, load_sem.at[i])
        for i, (src, dst) in enumerate((
            (w_key, wk_v), (w_value, wv_v), (w_out, wo_v), (gain, gain_v),
            (small, small_v), (start_angles.at[s], start_v),
            (w_query, wq_v), (w_pool, wp_v), (row_angles, angles_v),
        ))
    ]
    blocks = rows // QB
    tok_loads = [
        pltpu.make_async_copy(
            tokens.at[pl.ds(i * QB, QB)], tok.at[pl.ds(i * QB, QB)], tok_sem.at[i]
        )
        for i in range(blocks)
    ]
    for load in loads[:6]:
        load.start()
    for load in tok_loads:
        load.start()
    for load in loads[6:]:
        load.start()
    for load in loads[:6]:
        load.wait()

    lane = lax.broadcasted_iota(jnp.int32, (1, 2 * HEAD), 1)

    def swap_halves(value):
        return pltpu.roll(value, HEAD, 1)

    wk_f, wv_f = wk_v[...].astype(F32), wv_v[...].astype(F32)
    low_head = t < n_tp // 2
    k_part = jnp.where(low_head, wk_f, swap_halves(wk_f))
    v_part = jnp.where(low_head, swap_halves(wv_f), wv_f)
    kv_piece = jnp.where(lane < HEAD, k_part, v_part)
    half_rows = kv_piece.shape[0] // 2
    kvbuf[c, b, a] = jnp.where(c == 0, kv_piece[:half_rows], kv_piece[half_rows:]).astype(BF16)
    width = wo_v.shape[1]
    unit = (
        lax.broadcasted_iota(jnp.int32, (width, width), 0)
        == lax.broadcasted_iota(jnp.int32, (width, width), 1)
    ).astype(BF16)
    wbuf[c, b, a, x] = lax.dot_general(
        unit, wo_v[...], (((1,), (1,)), ((), ())), preferred_element_type=F32
    ).astype(BF16)

    features = tok.shape[1]
    chunk = 16

    def norm_block(first, count):
        def norm_rows(i, carry):
            at = pl.ds(pl.multiple_of(first + i * chunk, chunk), chunk)
            values = tok[at, :].astype(F32)
            center = jnp.sum(values, axis=-1, keepdims=True) * (1.0 / features)
            shifted = values - center
            spread = jnp.sum(shifted * shifted, axis=-1, keepdims=True) * (1.0 / features)
            tok[at, :] = (shifted * lax.rsqrt(spread + 1e-06) * gain_v[...]).astype(BF16)
            return carry

        lax.fori_loop(0, count // chunk, norm_rows, 0, unroll=2)

    def norm_blocks(lo, hi):
        for i in range(lo, hi):
            tok_loads[i].wait()
        norm_block(lo * QB, (hi - lo) * QB)

    norm_blocks(0, 2)

    pl.semaphore_wait(barrier, len(peers))
    own_kv = kvbuf.at[c, b, a]
    kv1 = [remote(own_kv, own_kv, kv1_s.at[k], kv1_r.at[k], along_a(k)) for k in range(1, RING)]
    for k in ORDER:
        kv1[k - 1].start()
    own_w = wbuf.at[c, b, a, x]
    w1 = [remote(own_w, own_w, w1_s.at[k], w1_r.at[k], along_x(k)) for k in range(1, 4)]
    for copy in w1:
        copy.start()

    norm_blocks(2, blocks)

    def arrived(dst, ssem, rsem):
        remote(dst, dst, ssem, rsem, (s, other)).wait_recv()

    for k in range(1, 4):
        arrived(wbuf.at[c, b, a, (x + 4 - k) % 4], w1_s.at[k], w1_r.at[k])
    row_w = wbuf.at[c, b, a]
    w2 = [remote(row_w, row_w, w2_s.at[k], w2_r.at[k], along_a(k)) for k in range(1, RING)]
    for k in ORDER:
        w2[k - 1].start()

    for load in loads[6:]:
        load.wait()

    def merge_rows(i, carry):
        at = pl.ds(pl.multiple_of(i * 256, 256), 256)
        wqp[at, :] = jnp.concatenate([wq_v[at, :], wp_v[at, :]], axis=1)
        return carry

    lax.fori_loop(0, features // 256, merge_rows, 0)

    def rotated(value, first):
        at = pl.ds(first, QB)
        row_c, row_s = angles_v[0, at, :], angles_v[1, at, :]
        base_c, base_s = start_v[0:1, :], start_v[1:2, :]
        cosine = base_c * row_c - base_s * row_s
        sine = base_s * row_c + base_c * row_s
        partner = jnp.where(
            lane < HEAD // 2,
            pltpu.roll(value, 2 * HEAD - HEAD // 2, 1),
            pltpu.roll(value, HEAD // 2, 1),
        )
        return value * cosine + partner * sine

    def query_block(i, carry):
        first = pl.multiple_of(i * QB, QB)
        value = jnp.dot(tok[pl.ds(first, QB), :], wqp[...], preferred_element_type=F32)
        p_ext[pl.ds(pl.multiple_of(EDGE + first, EDGE), QB), :] = value.astype(BF16)
        turned = rotated(value, first)
        q_v[pl.ds(first, QB), :] = jnp.where(lane < HEAD, turned, 0.0).astype(BF16)
        return carry

    lax.fori_loop(0, blocks, query_block, 0)

    low_edge, high_edge = p_ext.at[pl.ds(EDGE, EDGE)], p_ext.at[pl.ds(rows, EDGE)]
    ph = [
        remote(high_edge, p_ext.at[pl.ds(0, EDGE)], ph_s.at[0], ph_r.at[0], after),
        remote(low_edge, p_ext.at[pl.ds(EDGE + rows, EDGE)], ph_s.at[1], ph_r.at[1], before),
    ]
    for k in ORDER:
        arrived(kvbuf.at[c, b, (a + RING - k) % RING], kv1_s.at[k], kv1_r.at[k])
    line_kv = kvbuf.at[c, b]
    kv2 = [remote(line_kv, line_kv, kv2_s.at[k], kv2_r.at[k], along_b(k)) for k in range(1, RING)]
    for k in ORDER:
        kv2[k - 1].start()
    kvd = []
    for k in range(RING):
        part = kvbuf.at[c, (b + RING - k) % RING]
        kvd.append(remote(part, part, kvd_s.at[k], kvd_r.at[k], (s, other)))
    kvd[0].start()
    for copy in ph:
        copy.start()
    ph[0].wait_recv()
    ph[1].wait_recv()

    seq_total = n_sp * rows
    reach = 1 + (t // 2 > 0) + 2 * (t // 2 > 1) + 4 * (t // 2 > 2)
    span = QB + 2 * EDGE
    place = lax.broadcasted_iota(jnp.int32, (QB, span), 1) - EDGE
    apart = place - lax.broadcasted_iota(jnp.int32, (QB, span), 0)
    near = (apart >= -reach) & (apart < reach)
    row_id = lax.broadcasted_iota(jnp.int32, (QB, 1), 0)
    scale = small_v[0:1, :]
    sink = small_v[1:2, 0:1]

    def pool_block(i, carry):
        first = pl.multiple_of(i * QB, QB)
        inside = place + (s * rows + first)
        band = jnp.where(near & (inside >= 0) & (inside < seq_total), 1.0, 0.0).astype(BF16)
        sums = jnp.dot(band, p_ext[pl.ds(first, span), :], preferred_element_type=F32)
        position = row_id + (s * rows + first)
        counted = (
            jnp.minimum(position + reach, seq_total) - jnp.maximum(position - reach, 0)
        ).astype(F32)
        here = p_ext[pl.ds(pl.multiple_of(EDGE + first, EDGE), QB), :].astype(F32)
        pooled = (sums / counted - here) * scale
        pool_v[pl.ds(first, QB), :] = swap_halves(pooled).astype(BF16)
        return carry

    lax.fori_loop(0, blocks, pool_block, 0)

    for k in ORDER:
        arrived(wbuf.at[c, b, (a + RING - k) % RING], w2_s.at[k], w2_r.at[k])
    line_w = wbuf.at[c, b]
    w3 = [remote(line_w, line_w, w3_s.at[k], w3_r.at[k], along_b(k)) for k in range(1, RING)]
    wd = []
    for k in range(RING):
        part = wbuf.at[c, (b + RING - k) % RING]
        wd.append(remote(part, part, wd_s.at[k], wd_r.at[k], (s, other)))

    for k in ORDER:
        arrived(kvbuf.at[c, (b + RING - k) % RING], kv2_s.at[k], kv2_r.at[k])
        kvd[k].start()
    for k in ORDER:
        w3[k - 1].start()
    for k in (0, *ORDER):
        arrived(kvbuf.at[1 - c, (a + RING - k) % RING], kvd_s.at[k], kvd_r.at[k])
    wd[0].start()

    def join_rows(i, carry):
        for j in range(RING):
            at = pl.multiple_of((i * RING + j) * 2 * half_rows, 2 * half_rows)
            wkv[pl.ds(at, half_rows), :] = kvbuf[0, i, j]
            wkv[pl.ds(pl.multiple_of(at + half_rows, half_rows), half_rows), :] = kvbuf[1, j, i]
        return carry

    lax.fori_loop(0, RING, join_rows, 0)

    def key_block(i, carry):
        first = pl.multiple_of(i * QB, QB)
        value = jnp.dot(tok[pl.ds(first, QB), :], wkv[...], preferred_element_type=F32)
        kv_ext[pl.ds(pl.multiple_of(WINDOW + first, QB), QB), :] = rotated(value, first).astype(BF16)
        return carry

    key_block(0, 0)
    key_block(blocks - 1, 0)
    key_block(1, 0)
    kh = [
        remote(
            kv_ext.at[pl.ds(rows, WINDOW)], kv_ext.at[pl.ds(0, WINDOW)],
            kh_s.at[0], kh_r.at[0], after,
        ),
        remote(
            kv_ext.at[pl.ds(WINDOW, WINDOW)], kv_ext.at[pl.ds(WINDOW + rows, WINDOW)],
            kh_s.at[1], kh_r.at[1], before,
        ),
    ]
    for copy in kh:
        copy.start()
    lax.fori_loop(2, blocks - 1, key_block, 0)

    query_at = lax.broadcasted_iota(jnp.int32, (QB, QB), 0)
    key_at = lax.broadcasted_iota(jnp.int32, (QB, QB), 1)

    def attend(i):
        first = pl.multiple_of(i * QB, QB)
        keys = kv_ext[pl.ds(first, QB + 2 * WINDOW), :]
        scores = lax.dot_general(
            q_v[pl.ds(first, QB), :], keys, (((1,), (1,)), ((), ())), preferred_element_type=F32
        ) * HEAD ** (-0.5)
        begin = s * rows + first
        low_ok = (key_at >= query_at) & (key_at + (begin - WINDOW) >= 0)
        high_ok = (key_at <= query_at) & (key_at + (begin + QB) < seq_total)
        scores = jnp.concatenate(
            [
                jnp.where(low_ok, scores[:, :QB], NEG_BIG),
                scores[:, QB : 2 * QB],
                jnp.where(high_ok, scores[:, 2 * QB :], NEG_BIG),
            ],
            axis=1,
        )
        highest = jnp.maximum(jnp.max(scores, axis=-1, keepdims=True), sink)
        expo = jnp.exp(scores - highest)
        total = jnp.sum(expo, axis=-1, keepdims=True) + jnp.exp(sink - highest)
        weights = (expo * (1.0 / total)).astype(BF16)
        result = jnp.dot(weights, keys, preferred_element_type=F32)
        mix_send[i] = jnp.where(lane < HEAD, pool_v[pl.ds(first, QB), :].astype(F32), result).astype(BF16)

    def mix_copy(i):
        return remote(mix_send.at[i], mix_recv.at[t], mx_s.at[i], mx_r.at[t], (s, i))

    def hand_over(i):
        @pl.when(i != t)
        def _():
            mix_copy(i).start()

        @pl.when(i == t)
        def _():
            mix_recv[i] = mix_send[i]

    def inner(i, carry):
        attend(i)
        hand_over(i)
        return carry

    lax.fori_loop(1, blocks - 1, inner, 0)
    kh[0].wait_recv()
    attend(0)
    hand_over(0)
    kh[1].wait_recv()
    attend(blocks - 1)
    hand_over(blocks - 1)

    for k in ORDER:
        arrived(wbuf.at[c, (b + RING - k) % RING], w3_s.at[k], w3_r.at[k])
        wd[k].start()

    for k in range(1, n_tp):
        source = (t + k) % n_tp
        remote(mix_recv.at[source], mix_recv.at[source], mx_s.at[source], mx_r.at[source], (s, other)).wait_recv()
    left, right = [], []
    for j in range(n_tp // 2):
        even, odd = mix_recv[2 * j].astype(F32), mix_recv[2 * j + 1].astype(F32)
        left.append(jnp.where(lane < HEAD, swap_halves(even), odd).astype(BF16))
        right.append(jnp.where(lane < HEAD, even, swap_halves(odd)).astype(BF16))
    mixed = jnp.concatenate(left + right, axis=1)

    for k in (0, *ORDER):
        arrived(wbuf.at[1 - c, (a + RING - k) % RING], wd_s.at[k], wd_r.at[k])

    span_out = RING * width
    for i in range(RING):
        parts = []
        for j in range(4):
            parts.append(wbuf[0, i, :, j].reshape(span_out, QB))
            parts.append(wbuf[1, :, i, j].reshape(span_out, QB))
        out[:, i * span_out : (i + 1) * span_out] = lax.dot_general(
            mixed, jnp.concatenate(parts, axis=1), (((1,), (1,)), ((), ())),
            preferred_element_type=F32,
        ).astype(BF16)

    for copy in (*kv1, *kv2, *kvd, *w1, *w2, *w3, *wd, *ph, *kh):
        copy.wait_send()
    for i in range(blocks):
        @pl.when(i != t)
        def _():
            mix_copy(i).wait_send()


def body(tokens, norm_gain, w_query, w_key, w_value, w_pool_in, sink_logit, pool_scale, w_out):
    rows, features = tokens.shape
    n_sp, n_tp = lax.axis_size("sp"), lax.axis_size("tp")
    start, row = angle_tables(n_sp, rows)
    small = jnp.concatenate(
        [
            jnp.pad(pool_scale[None, :], ((0, 0), (HEAD, 0))),
            jnp.broadcast_to(sink_logit[:, None], (7, 2 * HEAD)),
        ],
        axis=0,
    )
    dma, vmem = pltpu.SemaphoreType.DMA, pltpu.VMEM
    half = w_key.shape[0] // 2
    width = w_out.shape[1]
    pair = 2 * HEAD
    scratch = [
        vmem((rows, features), BF16),
        vmem((1, features), F32),
        vmem(w_query.shape, BF16),
        vmem(w_pool_in.shape, BF16),
        vmem(w_key.shape, BF16),
        vmem(w_value.shape, BF16),
        vmem(w_out.shape, BF16),
        vmem((8, pair), F32),
        vmem((8, pair), F32),
        vmem((2, rows, pair), F32),
        vmem((features, pair), BF16),
        vmem((2, RING, RING, half, pair), BF16),
        vmem((features, pair), BF16),
        vmem((2, RING, RING, n_tp // 2, width, w_out.shape[0]), BF16),
        vmem((rows, pair), BF16),
        vmem((rows + 2 * EDGE, pair), BF16),
        vmem((rows, pair), BF16),
        vmem((rows + 2 * WINDOW, pair), BF16),
        vmem((n_tp, QB, pair), BF16),
        vmem((n_tp, QB, pair), BF16),
        dma((9,)),
        dma((rows // QB,)),
    ]
    counts = (8, 8, 8, 8, 8, 8, 4, 4, 8, 8, 8, 8, 8, 8, 2, 2, 2, 2, 8, 8)
    scratch += [dma((n,)) for n in counts]
    return pl.pallas_call(
        functools.partial(kernel, rows),
        name="mixer",
        out_shape=jax.ShapeDtypeStruct((rows // n_tp, w_out.shape[1] * n_sp), BF16),
        in_specs=[pl.BlockSpec(memory_space=pl.ANY)] * 10,
        out_specs=pl.BlockSpec(memory_space=pltpu.VMEM),
        scratch_shapes=scratch,
        compiler_params=pltpu.CompilerParams(
            collective_id=0, has_side_effects=True, vmem_limit_bytes=60 * 2**20
        ),
    )(
        tokens, norm_gain[None, :], w_query, w_key, w_value, w_pool_in, small, w_out,
        jnp.asarray(start), jnp.asarray(row),
    )


def solution(mesh):
    in_specs = (
        P("sp", None),
        P(),
        P(None, "tp"),
        P("sp", None),
        P("sp", None),
        P(None, "tp"),
        P("tp"),
        P("tp"),
        P("tp", "sp"),
    )
    out_specs = P(("sp", "tp"), None)
    return jax.shard_map(body, mesh=mesh, in_specs=in_specs, out_specs=out_specs, check_vma=False)
```

```python
import functools

import jax
import jax.numpy as jnp
import numpy as np
from jax import lax
from jax.experimental import pallas as pl
from jax.experimental.pallas import tpu as pltpu
from jax.sharding import PartitionSpec as P

HEAD = 64
WINDOW = 128
QB = 128
NEG_BIG = -1e30
EDGE = 16
RING = 8
ORDER = (1, 7, 2, 6, 3, 5, 4)
MESH = pl.DeviceIdType.MESH
F32 = jnp.float32
BF16 = jnp.bfloat16


def angle_tables(n_sp, rows):
    half = HEAD // 2
    inverse = np.float32(10000.0) ** (-np.arange(half, dtype=np.float32) / np.float32(half))

    def pair(positions):
        angles = positions[:, None].astype(np.float64) * inverse[None, :].astype(np.float64)
        cosine, sine = np.cos(angles), np.sin(angles)
        ones = np.ones((len(positions), HEAD))
        c = np.concatenate([cosine, cosine, ones], axis=1)
        s = np.concatenate([-sine, sine, 0.0 * ones], axis=1)
        return c.astype(np.float32), s.astype(np.float32)

    def cut(value):
        scale = np.exp2(np.floor(np.log2(np.where(value == 0, 1.0, np.abs(value)))) - 7)
        return np.trunc(value / scale) * scale

    exact = inverse.astype(np.float64)
    pieces = [cut(exact)]
    pieces.append(cut(exact - pieces[0]))
    pieces.append(exact - pieces[0] - pieces[1])
    start = np.zeros((n_sp, 8, 2 * HEAD), np.float32)
    start[:, 0], start[:, 1] = pair(np.arange(n_sp) * rows)
    start[:, 2, :half], start[:, 2, half:HEAD] = -1.0, 1.0
    for row, value in zip(range(3, 7), (*pieces, exact)):
        start[:, row, :HEAD] = np.concatenate([value, value])
    return start, np.stack(pair(np.arange(rows)))


def kernel(
    rows,
    tokens,
    gain,
    w_query,
    w_key,
    w_value,
    w_pool,
    scale,
    sink,
    w_out,
    start_angles,
    row_angles,
    out,
    tok,
    nrm,
    gain_v,
    wk_v,
    wv_v,
    scale_v,
    sink_v,
    start_v,
    angles_v,
    wqp,
    kvbuf,
    wkv,
    wbuf,
    q_v,
    p_ext,
    pool_v,
    kv_ext,
    mix_send,
    mix_recv,
    load_sem,
    tok_sem,
    kv1_s,
    kv1_r,
    kv2_s,
    kv2_r,
    kvd_s,
    kvd_r,
    w1_s,
    w1_r,
    w2_s,
    w2_r,
    w3_s,
    w3_r,
    wd_s,
    wd_r,
    ph_s,
    ph_r,
    kh_s,
    kh_r,
    mx_s,
    mx_r,
):
    s = lax.axis_index("sp")
    t = lax.axis_index("tp")
    n_sp = lax.axis_size("sp")
    n_tp = lax.axis_size("tp")
    x, c = t // 2, t % 2
    z, y = s // RING, s % RING
    a = y + c * (z - y)
    b = z + c * (y - z)
    step_a = 1 + (RING - 1) * c
    step_b = RING - (RING - 1) * c
    other = t + 1 - 2 * c

    def along_a(k):
        return (s + ((a + k) % RING - a) * step_a, t)

    def along_b(k):
        return (s + ((b + k) % RING - b) * step_b, t)

    def along_x(k):
        return (s, ((x + k) % 4) * 2 + c)

    def along_tp(k):
        return (s, (t + k) % n_tp)

    after = ((s + 1) % n_sp, t)
    before = ((s + n_sp - 1) % n_sp, t)

    barrier = pltpu.get_barrier_semaphore()
    peers = (
        [along_a(k) for k in range(1, RING)]
        + [along_b(k) for k in range(1, RING)]
        + [along_tp(k) for k in range(1, n_tp)]
        + [after, before]
    )
    for peer in peers:
        pl.semaphore_signal(barrier, inc=1, device_id=peer, device_id_type=MESH)

    def remote(src, dst, ssem, rsem, device):
        return pltpu.make_async_remote_copy(
            src_ref=src, dst_ref=dst, send_sem=ssem, recv_sem=rsem,
            device_id=device, device_id_type=MESH,
        )

    loads = [
        pltpu.make_async_copy(src, dst, load_sem.at[i])
        for i, (src, dst) in enumerate((
            (w_key, wk_v), (w_value, wv_v), (w_out, wbuf.at[c, b, a, x]), (gain, gain_v),
            (w_query, wqp.at[pl.ds(0, HEAD)]), (w_pool, wqp.at[pl.ds(HEAD, HEAD)]),
            (row_angles, angles_v), (start_angles.at[s], start_v), (scale, scale_v), (sink, sink_v),
        ))
    ]
    blocks = rows // QB
    tok_loads = [
        pltpu.make_async_copy(
            tokens.at[pl.ds(i * QB, QB)], tok.at[pl.ds(i * QB, QB)], tok_sem.at[i]
        )
        for i in range(blocks)
    ]
    for load in loads[:3]:
        load.start()
    for load in tok_loads:
        load.start()
    for load in loads[3:]:
        load.start()
    with jax.named_scope("load_wait"):
        for load in loads[:3]:
            load.wait()

    lane = lax.broadcasted_iota(jnp.int32, (1, 2 * HEAD), 1)

    def swap_halves(value):
        return pltpu.roll(value, HEAD, 1)

    wk_f, wv_f = wk_v[...].astype(F32), wv_v[...].astype(F32)
    low_head = t < n_tp // 2
    k_part = jnp.where(low_head, wk_f, swap_halves(wk_f))
    v_part = jnp.where(low_head, swap_halves(wv_f), wv_f)
    kv_piece = jnp.where(lane < HEAD, k_part, v_part)
    half_rows = kv_piece.shape[0] // 2
    kvbuf[c, b, a] = jnp.where(c == 0, kv_piece[:half_rows], kv_piece[half_rows:]).astype(BF16)
    width = wbuf.shape[4]

    with jax.named_scope("barrier_wait"):
        pl.semaphore_wait(barrier, len(peers))

    own_w = wbuf.at[c, b, a, x]
    w1 = [remote(own_w, own_w, w1_s.at[k], w1_r.at[k], along_x(k)) for k in range(1, 4)]
    for copy in w1:
        copy.start()
    own_kv = kvbuf.at[c, b, a]
    kv1 = [remote(own_kv, own_kv, kv1_s.at[k], kv1_r.at[k], along_a(k)) for k in range(1, RING)]
    for k in ORDER:
        kv1[k - 1].start()

    features = tok.shape[1]
    chunk, slab = 32, 128

    def slabs():
        return [slice(j * slab, (j + 1) * slab) for j in range(features // slab)]

    def norm_at(i):
        return pl.ds(pl.multiple_of(i * chunk, chunk), chunk)

    def norm_center(i):
        parts = [tok[norm_at(i), cols].astype(F32) for cols in slabs()]
        while len(parts) > 1:
            parts = [p + q for p, q in zip(parts[::2], parts[1::2])]
        return jnp.sum(parts[0], axis=-1, keepdims=True) * (1.0 / features)

    def norm_spread(i, center):
        total = [0.0, 0.0]
        for j, cols in enumerate(slabs()):
            shifted = tok[norm_at(i), cols].astype(F32) - center
            total[j % 2] = total[j % 2] + shifted * shifted
        spread = jnp.sum(total[0] + total[1], axis=-1, keepdims=True) * (1.0 / features)
        return lax.rsqrt(spread + 1e-06)

    def norm_store(i, center, inverse):
        for cols in slabs():
            shifted = tok[norm_at(i), cols].astype(F32) - center
            nrm[norm_at(i), cols] = (shifted * inverse * gain_v[:, cols]).astype(BF16)

    def norm_rows(lo, hi):
        def step(i, carry):
            later, center, inverse = carry
            norm_store(i, center, inverse)
            ahead = jnp.minimum(i + 1, hi - 1)
            next_inverse = norm_spread(ahead, later)
            return norm_center(jnp.minimum(i + 2, hi - 1)), later, next_inverse

        first = norm_center(lo)
        lax.fori_loop(lo, hi, step, (norm_center(lo + 1), first, norm_spread(lo, first)))

    def norm_blocks(lo, hi):
        for i in range(lo, hi):
            tok_loads[i].wait()
        norm_rows(lo * QB // chunk, hi * QB // chunk)

    def arrived(dst, ssem, rsem):
        remote(dst, dst, ssem, rsem, (s, other)).wait_recv()

    loads[3].wait()
    with jax.named_scope("norm_first"):
        norm_blocks(0, blocks // 2)
    with jax.named_scope("w1_wait"):
        for k in range(1, 4):
            arrived(wbuf.at[c, b, a, (x + 4 - k) % 4], w1_s.at[k], w1_r.at[k])
    row_w = wbuf.at[c, b, a]
    w2 = [remote(row_w, row_w, w2_s.at[k], w2_r.at[k], along_a(k)) for k in range(1, RING)]
    for k in ORDER:
        w2[k - 1].start()
    with jax.named_scope("norm_rest"):
        norm_blocks(blocks // 2, blocks)
    with jax.named_scope("kv1_wait"):
        for k in ORDER:
            arrived(kvbuf.at[c, b, (a + RING - k) % RING], kv1_s.at[k], kv1_r.at[k])
    line_kv = kvbuf.at[c, b]
    kv2 = [remote(line_kv, line_kv, kv2_s.at[k], kv2_r.at[k], along_b(k)) for k in range(1, RING)]
    for k in ORDER:
        kv2[k - 1].start()
    kvd = []
    for k in range(RING):
        part = kvbuf.at[c, (b + RING - k) % RING]
        kvd.append(remote(part, part, kvd_s.at[k], kvd_r.at[k], (s, other)))
    kvd[0].start()
    for load in loads[4:]:
        load.wait()

    seq_total = n_sp * rows
    base_c, base_s = start_v[0:1, :], start_v[1:2, :]
    signed, piece_1, piece_2, piece_3, whole = (start_v[i : i + 1, :] for i in range(2, 7))
    turn_rows = 64

    def turn_block(i, carry):
        at = pl.ds(pl.multiple_of(i * turn_rows, turn_rows), turn_rows)
        row_c, row_s = angles_v[0, at, :], angles_v[1, at, :]
        cosine = base_c * row_c - base_s * row_s
        sine = base_s * row_c + base_c * row_s
        position = (
            lax.broadcasted_iota(jnp.int32, (turn_rows, 1), 0) + (s * rows + i * turn_rows)
        ).astype(F32)
        rounding = position * whole - position * piece_1
        rounding = rounding - position * piece_2 - position * piece_3
        rounding = rounding * signed
        angles_v[0, at, :] = cosine - rounding * sine
        angles_v[1, at, :] = sine + rounding * cosine
        return carry

    with jax.named_scope("turns"):
        lax.fori_loop(0, rows // turn_rows, turn_block, 0)

    def rotated(value, at):
        partner = jnp.where(
            lane < HEAD // 2,
            pltpu.roll(value, 2 * HEAD - HEAD // 2, 1),
            pltpu.roll(value, HEAD // 2, 1),
        )
        return value * angles_v[0, at, :] + partner * angles_v[1, at, :]

    wide = 2 * QB

    def query_block(i, carry):
        at = pl.ds(pl.multiple_of(i * wide, wide), wide)
        value = lax.dot_general(
            nrm[at, :], wqp[...], (((1,), (1,)), ((), ())), preferred_element_type=F32
        )
        p_ext[pl.ds(pl.multiple_of(EDGE + i * wide, EDGE), wide), :] = value.astype(BF16)
        q_v[at, :] = jnp.where(lane < HEAD, rotated(value, at), 0.0).astype(BF16)
        return carry

    with jax.named_scope("query_proj"):
        lax.fori_loop(0, rows // wide, query_block, 0)

    low_edge, high_edge = p_ext.at[pl.ds(EDGE, EDGE)], p_ext.at[pl.ds(rows, EDGE)]
    ph = [
        remote(high_edge, p_ext.at[pl.ds(0, EDGE)], ph_s.at[0], ph_r.at[0], after),
        remote(low_edge, p_ext.at[pl.ds(EDGE + rows, EDGE)], ph_s.at[1], ph_r.at[1], before),
    ]
    for copy in ph:
        copy.start()

    with jax.named_scope("w2_wait"):
        for k in ORDER:
            arrived(wbuf.at[c, b, (a + RING - k) % RING], w2_s.at[k], w2_r.at[k])

    half_line = RING // 2

    def half_at(owner, place, u):
        return wbuf.at[owner, place, pl.ds(half_line * u, half_line)]

    def to_right(d, u):
        part = half_at(c, (b + RING - d) % RING, u)
        return remote(part, part, w3_s.at[0, 2 * d + u], w3_r.at[0, 2 * d + u], along_b(1))

    def to_left(d, u):
        part = half_at(c, (b + d) % RING, u)
        return remote(part, part, w3_s.at[1, 2 * d + u], w3_r.at[1, 2 * d + u], along_b(RING - 1))

    def across(way, d, u):
        part = half_at(c, (b + (RING - d if way == 0 else d)) % RING, u)
        index = 2 * d + u
        return remote(part, part, wd_s.at[way, index], wd_r.at[way, index], (s, other))

    ring_copies, cross_copies = [], []

    def launch(copy, into):
        copy.start()
        into.append(copy)

    for u in range(2):
        launch(to_right(0, u), ring_copies)
        launch(to_left(0, u), ring_copies)
        launch(across(u, 0, u), cross_copies)

    ring_steps = [((d, u), (d, u)) for d in (1, 2, 3) for u in (0, 1)] + [((4, 0), (4, 1))]

    def ring_advance(step):
        with jax.named_scope("ring_wait"):
            for way, (d, u) in enumerate(ring_steps[step]):
                send = to_right if way == 0 else to_left
                place = (b + (RING - d if way == 0 else d)) % RING
                index = 2 * (d - 1) + u
                arrived(half_at(c, place, u), w3_s.at[way, index], w3_r.at[way, index])
                if d < 3 or (d == 3 and u == way):
                    launch(send(d, u), ring_copies)
                launch(across(way, d, u), cross_copies)

    reach = 1 + (t // 2 > 0) + 2 * (t // 2 > 1) + 4 * (t // 2 > 2)
    span = QB + 2 * EDGE
    place = lax.broadcasted_iota(jnp.int32, (QB, span), 1) - EDGE
    apart = place - lax.broadcasted_iota(jnp.int32, (QB, span), 0)
    near = (apart >= -reach) & (apart < reach)
    row_id = lax.broadcasted_iota(jnp.int32, (QB, 1), 0)
    scales = jnp.concatenate([scale_v[...], scale_v[...]], axis=1)
    sinks = sink_v[...]

    def pool_block(i, carry):
        first = pl.multiple_of(i * QB, QB)
        inside = place + (s * rows + first)
        band = jnp.where(near & (inside >= 0) & (inside < seq_total), 1.0, 0.0).astype(BF16)
        sums = jnp.dot(band, p_ext[pl.ds(first, span), :], preferred_element_type=F32)
        position = row_id + (s * rows + first)
        counted = (
            jnp.minimum(position + reach, seq_total) - jnp.maximum(position - reach, 0)
        ).astype(F32)
        here = p_ext[pl.ds(pl.multiple_of(EDGE + first, EDGE), QB), :].astype(F32)
        pooled = (sums / counted - here) * scales
        pool_v[pl.ds(first, QB), :] = swap_halves(pooled).astype(BF16)
        return carry

    with jax.named_scope("pool_halo"):
        ph[0].wait_recv()
        ph[1].wait_recv()
    with jax.named_scope("pool_mix"):
        lax.fori_loop(0, blocks, pool_block, 0)

    with jax.named_scope("kv2_wait"):
        for k in ORDER:
            arrived(kvbuf.at[c, (b + RING - k) % RING], kv2_s.at[k], kv2_r.at[k])
            kvd[k].start()
    with jax.named_scope("kvd_wait"):
        for k in (0, *ORDER):
            arrived(kvbuf.at[1 - c, (a + RING - k) % RING], kvd_s.at[k], kvd_r.at[k])

    def join_rows(i, carry):
        for j in range(RING):
            at = pl.multiple_of((i * RING + j) * 2 * half_rows, 2 * half_rows)
            wkv[pl.ds(at, half_rows), :] = kvbuf[0, i, j]
            wkv[pl.ds(pl.multiple_of(at + half_rows, half_rows), half_rows), :] = kvbuf[1, j, i]
        return carry

    with jax.named_scope("kv_join"):
        lax.fori_loop(0, RING, join_rows, 0)

    def key_rows(first, count):
        at = pl.ds(pl.multiple_of(first, QB), count)
        value = jnp.dot(nrm[at, :], wkv[...], preferred_element_type=F32)
        kv_ext[pl.ds(pl.multiple_of(WINDOW + first, QB), count), :] = rotated(value, at).astype(BF16)

    with jax.named_scope("key_edge"):
        key_rows(0, QB)
        key_rows(rows - QB, QB)
    ring_advance(0)
    kh = [
        remote(
            kv_ext.at[pl.ds(rows, WINDOW)], kv_ext.at[pl.ds(0, WINDOW)],
            kh_s.at[0], kh_r.at[0], after,
        ),
        remote(
            kv_ext.at[pl.ds(WINDOW, WINDOW)], kv_ext.at[pl.ds(WINDOW + rows, WINDOW)],
            kh_s.at[1], kh_r.at[1], before,
        ),
    ]
    for copy in kh:
        copy.start()

    def key_wide(i, carry):
        key_rows(QB + i * wide, wide)
        return carry

    with jax.named_scope("key_rest"):
        lax.fori_loop(0, (rows - 2 * QB) // wide, key_wide, 0)
    ring_advance(1)

    query_at = lax.broadcasted_iota(jnp.int32, (QB, QB), 0)
    key_at = lax.broadcasted_iota(jnp.int32, (QB, QB), 1)

    def attend(i):
        first = pl.multiple_of(i * QB, QB)
        keys = kv_ext[pl.ds(first, QB + 2 * WINDOW), :]
        scores = lax.dot_general(
            q_v[pl.ds(first, QB), :], keys, (((1,), (1,)), ((), ())), preferred_element_type=F32
        ) * HEAD ** (-0.5)
        begin = s * rows + first
        low_ok = (key_at >= query_at) & (key_at + (begin - WINDOW) >= 0)
        high_ok = (key_at <= query_at) & (key_at + (begin + QB) < seq_total)
        scores = jnp.concatenate(
            [
                jnp.where(low_ok, scores[:, :QB], NEG_BIG),
                scores[:, QB : 2 * QB],
                jnp.where(high_ok, scores[:, 2 * QB :], NEG_BIG),
            ],
            axis=1,
        )
        highest = jnp.maximum(jnp.max(scores, axis=-1, keepdims=True), sinks)
        expo = jnp.exp(scores - highest)
        total = jnp.sum(expo, axis=-1, keepdims=True) + jnp.exp(sinks - highest)
        weights = (expo * (1.0 / total)).astype(BF16)
        result = jnp.dot(weights, keys, preferred_element_type=F32)
        mix_send[i] = jnp.where(lane < HEAD, pool_v[pl.ds(first, QB), :].astype(F32), result).astype(BF16)

    def mix_copy(i):
        return remote(mix_send.at[i], mix_recv.at[t], mx_s.at[i], mx_r.at[t], (s, i))

    def hand_over(i):
        @pl.when(i != t)
        def _():
            mix_copy(i).start()

        @pl.when(i == t)
        def _():
            mix_recv[i] = mix_send[i]

    def attend_pair(i, j):
        with jax.named_scope("attend"):
            attend(i)
            attend(j)
        hand_over(i)
        hand_over(j)

    attend_pair(1, 2)
    ring_advance(2)
    attend_pair(3, 4)
    ring_advance(3)
    attend_pair(5, 6)
    ring_advance(4)
    with jax.named_scope("key_halo"):
        kh[0].wait_recv()
        kh[1].wait_recv()
    attend_pair(0, blocks - 1)
    ring_advance(5)
    ring_advance(6)

    with jax.named_scope("mix_wait"):
        for k in range(1, n_tp):
            source = (t + k) % n_tp
            remote(mix_recv.at[source], mix_recv.at[source], mx_s.at[source], mx_r.at[source], (s, other)).wait_recv()
    left, right = [], []
    for j in range(n_tp // 2):
        even, odd = mix_recv[2 * j].astype(F32), mix_recv[2 * j + 1].astype(F32)
        left.append(jnp.where(lane < HEAD, swap_halves(even), odd).astype(BF16))
        right.append(jnp.where(lane < HEAD, even, swap_halves(odd)).astype(BF16))
    mixed = jnp.concatenate(left + right, axis=1)

    with jax.named_scope("wd_wait"):
        for way in range(2):
            place = a
            arrived(half_at(1 - c, place, way), wd_s.at[way, way], wd_r.at[way, way])
        for step in ring_steps:
            for way, (d, u) in enumerate(step):
                place = (a + (RING - d if way == 0 else d)) % RING
                index = 2 * d + u
                arrived(half_at(1 - c, place, u), wd_s.at[way, index], wd_r.at[way, index])

    span_out = RING * width
    with jax.named_scope("out_proj"):
        for i in range(RING):
            parts = []
            for j in range(4):
                parts.append(wbuf[0, i, :, j].reshape(span_out, QB))
                parts.append(wbuf[1, :, i, j].reshape(span_out, QB))
            out[:, i * span_out : (i + 1) * span_out] = lax.dot_general(
                mixed, jnp.concatenate(parts, axis=1), (((1,), (1,)), ((), ())),
                preferred_element_type=F32,
            ).astype(BF16)

    with jax.named_scope("send_wait"):
        for copy in (*kv1, *kv2, *kvd, *w1, *w2, *ring_copies, *cross_copies, *ph, *kh):
            copy.wait_send()
    for i in range(blocks):
        @pl.when(i != t)
        def _():
            mix_copy(i).wait_send()


def body(tokens, norm_gain, w_query, w_key, w_value, w_pool_in, sink_logit, pool_scale, w_out):
    rows, features = tokens.shape
    n_sp, n_tp = lax.axis_size("sp"), lax.axis_size("tp")
    start, row = angle_tables(n_sp, rows)
    dma, vmem = pltpu.SemaphoreType.DMA, pltpu.VMEM
    half = w_key.shape[0] // 2
    width = w_out.shape[1]
    pair = 2 * HEAD
    scratch = [
        vmem((rows, features), BF16),
        vmem((rows, features), BF16),
        vmem((1, features), F32),
        vmem(w_key.shape, BF16),
        vmem(w_value.shape, BF16),
        vmem((1, HEAD), F32),
        vmem((1, 1), F32),
        vmem((8, pair), F32),
        vmem((2, rows, pair), F32),
        vmem((pair, features), BF16),
        vmem((2, RING, RING, half, pair), BF16),
        vmem((features, pair), BF16),
        vmem((2, RING, RING, n_tp // 2, width, w_out.shape[0]), BF16),
        vmem((rows, pair), BF16),
        vmem((rows + 2 * EDGE, pair), BF16),
        vmem((rows, pair), BF16),
        vmem((rows + 2 * WINDOW, pair), BF16),
        vmem((n_tp, QB, pair), BF16),
        vmem((n_tp, QB, pair), BF16),
        dma((10,)),
        dma((rows // QB,)),
    ]
    counts = (8, 8, 8, 8, 8, 8, 4, 4, 8, 8, (2, 8), (2, 8), (2, 10), (2, 10), 2, 2, 2, 2, 8, 8)
    scratch += [dma(n if isinstance(n, tuple) else (n,)) for n in counts]
    return pl.pallas_call(
        functools.partial(kernel, rows),
        name="mixer",
        out_shape=jax.ShapeDtypeStruct((rows // n_tp, w_out.shape[1] * n_sp), BF16),
        in_specs=[pl.BlockSpec(memory_space=pl.ANY)] * 11,
        out_specs=pl.BlockSpec(memory_space=pltpu.VMEM),
        scratch_shapes=scratch,
        compiler_params=pltpu.CompilerParams(
            collective_id=0, has_side_effects=True, vmem_limit_bytes=60 * 2**20
        ),
    )(
        tokens, norm_gain[None, :], w_query.T, w_key, w_value, w_pool_in.T, pool_scale[None, :], sink_logit[None, :], w_out.T,
        jnp.asarray(start), jnp.asarray(row),
    )


def solution(mesh):
    in_specs = (
        P("sp", None),
        P(),
        P(None, "tp"),
        P("sp", None),
        P("sp", None),
        P(None, "tp"),
        P("tp"),
        P("tp"),
        P("tp", "sp"),
    )
    out_specs = P(("sp", "tp"), None)
    return jax.shard_map(body, mesh=mesh, in_specs=in_specs, out_specs=out_specs, check_vma=False)
```

```python
import functools

import jax
import jax.numpy as jnp
import numpy as np
from jax import lax
from jax.experimental import pallas as pl
from jax.experimental.pallas import tpu as pltpu
from jax.sharding import PartitionSpec as P

HEAD = 64
WINDOW = 128
QB = 128
NEG_BIG = -1e30
EDGE = 16
RING = 8
ORDER = (1, 7, 2, 6, 3, 5, 4)
FAR_FIRST = (4, 5, 3, 6, 2, 7, 1)
MESH = pl.DeviceIdType.MESH
F32 = jnp.float32
BF16 = jnp.bfloat16


def angle_tables(n_sp, rows):
    half = HEAD // 2
    inverse = np.float32(10000.0) ** (-np.arange(half, dtype=np.float32) / np.float32(half))

    def pair(positions):
        angles = positions[:, None].astype(np.float64) * inverse[None, :].astype(np.float64)
        cosine, sine = np.cos(angles), np.sin(angles)
        ones = np.ones((len(positions), HEAD))
        c = np.concatenate([cosine, cosine, ones], axis=1)
        s = np.concatenate([-sine, sine, 0.0 * ones], axis=1)
        return c.astype(np.float32), s.astype(np.float32)

    def cut(value):
        scale = np.exp2(np.floor(np.log2(np.where(value == 0, 1.0, np.abs(value)))) - 7)
        return np.trunc(value / scale) * scale

    exact = inverse.astype(np.float64)
    pieces = [cut(exact)]
    pieces.append(cut(exact - pieces[0]))
    pieces.append(exact - pieces[0] - pieces[1])
    start = np.zeros((n_sp, 8, 2 * HEAD), np.float32)
    start[:, 0], start[:, 1] = pair(np.arange(n_sp) * rows)
    start[:, 2, :half], start[:, 2, half:HEAD] = -1.0, 1.0
    for row, value in zip(range(3, 7), (*pieces, exact)):
        start[:, row, :HEAD] = np.concatenate([value, value])
    return start, np.stack(pair(np.arange(rows)))


def kernel(
    rows,
    tokens,
    gain,
    w_query,
    w_key,
    w_value,
    w_pool,
    scale,
    sink,
    w_out,
    start_angles,
    row_angles,
    out,
    tok,
    nrm,
    gain_v,
    wk_v,
    wv_v,
    scale_v,
    sink_v,
    start_v,
    angles_v,
    wqp,
    kvbuf,
    wkv,
    wbuf,
    q_v,
    p_ext,
    pool_v,
    kv_ext,
    mix_send,
    mix_recv,
    load_sem,
    tok_sem,
    sent,
    got,
    x_sem,
    ring_sem,
):
    s = lax.axis_index("sp")
    t = lax.axis_index("tp")
    n_sp = lax.axis_size("sp")
    n_tp = lax.axis_size("tp")
    x, c = t // 2, t % 2
    z, y = s // RING, s % RING
    a = y + c * (z - y)
    b = z + c * (y - z)
    features = tok.shape[1]
    blocks = rows // QB
    half_blocks = blocks // 2

    def load(src, dst, i):
        return pltpu.make_async_copy(src, dst, load_sem.at[i])

    early = [
        load(w_key, wk_v, 0), load(w_value, wv_v, 1), load(w_out, wbuf.at[c, b, x, a], 2),
    ]
    late = [
        load(gain, gain_v, 3),
        load(w_query, wqp.at[pl.ds(0, HEAD)], 4), load(w_pool, wqp.at[pl.ds(HEAD, HEAD)], 5),
        load(row_angles, angles_v, 6), load(start_angles.at[s], start_v, 7),
        load(scale, scale_v, 8), load(sink, sink_v, 9),
    ]
    tok_loads = [
        pltpu.make_async_copy(
            tokens.at[pl.ds(i * QB, QB)], tok.at[pl.ds(i * QB, QB)], tok_sem.at[i]
        )
        for i in range(blocks)
    ]
    for copy in early:
        copy.start()

    step_a = 1 + (RING - 1) * c
    step_b = RING - (RING - 1) * c
    other = t + 1 - 2 * c

    def along_a(k):
        return (s + ((a + k) % RING - a) * step_a, t)

    def along_b(k):
        return (s + ((b + k) % RING - b) * step_b, t)

    def along_x(k):
        return (s, ((x + k) % 4) * 2 + c)

    def along_tp(k):
        return (s, (t + k) % n_tp)

    after = ((s + 1) % n_sp, t)
    before = ((s + n_sp - 1) % n_sp, t)

    barrier = pltpu.get_barrier_semaphore()
    peers = (
        [along_a(k) for k in ORDER]
        + [along_b(k) for k in ORDER]
        + [along_tp(k) for k in range(1, n_tp)]
        + [after, before]
    )
    for peer in peers:
        pl.semaphore_signal(barrier, inc=1, device_id=peer, device_id_type=MESH)
    for copy in (*tok_loads, *late):
        copy.start()

    def remote(src, dst, ssem, rsem, device):
        return pltpu.make_async_remote_copy(
            src_ref=src, dst_ref=dst, send_sem=ssem, recv_sem=rsem,
            device_id=device, device_id_type=MESH,
        )

    def landed(region, sem):
        remote(region, region, sem, sem, (s, other)).wait_recv()

    def left_here(region, sem):
        remote(region, region, sem, sem, (s, other)).wait_send()

    KV1, KV2, KVD, W1, W2, WD, PH, KH, MX, RR, RL = range(11)

    with jax.named_scope("load_wait"):
        for copy in early:
            copy.wait()

    lane = lax.broadcasted_iota(jnp.int32, (1, 2 * HEAD), 1)

    def swap_halves(value):
        return pltpu.roll(value, HEAD, 1)

    wk_f, wv_f = wk_v[...].astype(F32), wv_v[...].astype(F32)
    low_head = t < n_tp // 2
    k_part = jnp.where(low_head, wk_f, swap_halves(wk_f))
    v_part = jnp.where(low_head, swap_halves(wv_f), wv_f)
    kv_piece = jnp.where(lane < HEAD, k_part, v_part)
    half_rows = kv_piece.shape[0] // 2
    kvbuf[c, b, a] = jnp.where(c == 0, kv_piece[:half_rows], kv_piece[half_rows:]).astype(BF16)
    width = wbuf.shape[4]

    with jax.named_scope("barrier_wait"):
        pl.semaphore_wait(barrier, len(peers))

    own_kv, own_w = kvbuf.at[c, b, a], wbuf.at[c, b, x, a]
    for k in FAR_FIRST:
        remote(own_kv, own_kv, sent.at[KV1], got.at[KV1], along_a(k)).start()
    for k in FAR_FIRST:
        remote(own_w, own_w, sent.at[W1], got.at[W1], along_a(k)).start()

    chunk, slab = 32, 128

    def slabs():
        return [slice(j * slab, (j + 1) * slab) for j in range(features // slab)]

    def norm_at(i):
        return pl.ds(pl.multiple_of(i * chunk, chunk), chunk)

    def norm_center(i):
        parts = [tok[norm_at(i), cols].astype(F32) for cols in slabs()]
        while len(parts) > 1:
            parts = [p + q for p, q in zip(parts[::2], parts[1::2])]
        return jnp.sum(parts[0], axis=-1, keepdims=True) * (1.0 / features)

    def norm_spread(i, center):
        total = [0.0, 0.0]
        for j, cols in enumerate(slabs()):
            shifted = tok[norm_at(i), cols].astype(F32) - center
            total[j % 2] = total[j % 2] + shifted * shifted
        spread = jnp.sum(total[0] + total[1], axis=-1, keepdims=True) * (1.0 / features)
        return lax.rsqrt(spread + 1e-06)

    def norm_store(i, center, inverse):
        for cols in slabs():
            shifted = tok[norm_at(i), cols].astype(F32) - center
            nrm[norm_at(i), cols] = (shifted * inverse * gain_v[:, cols]).astype(BF16)

    def norm_blocks(lo, hi):
        for i in range(lo, hi):
            tok_loads[i].wait()
        lo, hi = lo * QB // chunk, hi * QB // chunk

        def step(i, carry):
            later, center, inverse = carry
            norm_store(i, center, inverse)
            next_inverse = norm_spread(jnp.minimum(i + 1, hi - 1), later)
            return norm_center(jnp.minimum(i + 2, hi - 1)), later, next_inverse

        first = norm_center(lo)
        lax.fori_loop(lo, hi, step, (norm_center(lo + 1), first, norm_spread(lo, first)))

    late[0].wait()
    with jax.named_scope("norm_a"):
        norm_blocks(0, half_blocks)
    with jax.named_scope("norm_b"):
        norm_blocks(half_blocks, half_blocks + 2)
    with jax.named_scope("kv1_wait"):
        landed(kvbuf.at[c, b, pl.ds(0, RING - 1)], got.at[KV1])
    line_kv = kvbuf.at[c, b]
    for k in FAR_FIRST:
        remote(line_kv, line_kv, sent.at[KV2], got.at[KV2], along_b(k)).start()
    with jax.named_scope("w1_wait"):
        landed(wbuf.at[c, b, x, pl.ds(0, RING - 1)], got.at[W1])

    def chunk_at(way, d):
        return (b + (RING - d if way == 0 else d)) % RING

    def part_at(owner, place, r):
        return wbuf.at[owner, place, (x + r) % 4]

    def ring_send(way, d, r):
        part = part_at(c, chunk_at(way, d), r)
        device = along_b(1 if way == 0 else RING - 1)
        remote(part, part, sent.at[RR + way], ring_sem.at[way, 4 * d + r], device).start()

    def cross(place, r):
        part = part_at(c, place, r)
        remote(part, part, sent.at[WD], got.at[WD], (s, other)).start()

    def ring_start(r):
        ring_send(0, 0, r)
        ring_send(1, 0, r)
        cross(b, r)

    def ring_advance(d, parts):
        with jax.named_scope("ring_wait"):
            for r in parts:
                for way in range(2):
                    if d == 4 and r // 2 != way:
                        continue
                    place = chunk_at(way, d)
                    landed(part_at(c, place, r), ring_sem.at[way, 4 * (d - 1) + r])
                    if d < 3 or (d == 3 and r // 2 == way):
                        ring_send(way, d, r)
                    cross(place, r)

    line_w = part_at(c, b, 0)
    for k in (2, 1, 3):
        remote(line_w, line_w, sent.at[W2], x_sem.at[k], along_x(k)).start()
    ring_start(0)

    with jax.named_scope("norm_c"):
        norm_blocks(half_blocks + 2, blocks)
    for copy in late[1:]:
        copy.wait()

    seq_total = n_sp * rows
    base_c, base_s = start_v[0:1, :], start_v[1:2, :]
    signed, piece_1, piece_2, piece_3, whole = (start_v[i : i + 1, :] for i in range(2, 7))
    turn_rows = 64

    def turn_block(i, carry):
        at = pl.ds(pl.multiple_of(i * turn_rows, turn_rows), turn_rows)
        row_c, row_s = angles_v[0, at, :], angles_v[1, at, :]
        cosine = base_c * row_c - base_s * row_s
        sine = base_s * row_c + base_c * row_s
        position = (
            lax.broadcasted_iota(jnp.int32, (turn_rows, 1), 0) + (s * rows + i * turn_rows)
        ).astype(F32)
        rounding = position * whole - position * piece_1
        rounding = rounding - position * piece_2 - position * piece_3
        rounding = rounding * signed
        angles_v[0, at, :] = cosine - rounding * sine
        angles_v[1, at, :] = sine + rounding * cosine
        return carry

    with jax.named_scope("turns"):
        lax.fori_loop(0, rows // turn_rows, turn_block, 0)

    def rotated(value, at):
        partner = jnp.where(
            lane < HEAD // 2,
            pltpu.roll(value, 2 * HEAD - HEAD // 2, 1),
            pltpu.roll(value, HEAD // 2, 1),
        )
        return value * angles_v[0, at, :] + partner * angles_v[1, at, :]

    wide = 2 * QB
    query_scale = jnp.where(lane < HEAD, HEAD ** (-0.5), 0.0)

    def query_block(i, carry):
        at = pl.ds(pl.multiple_of(i * wide, wide), wide)
        value = lax.dot_general(
            nrm[at, :], wqp[...], (((1,), (1,)), ((), ())), preferred_element_type=F32
        )
        p_ext[pl.ds(pl.multiple_of(EDGE + i * wide, EDGE), wide), :] = value.astype(BF16)
        q_v[at, :] = (rotated(value, at) * query_scale).astype(BF16)
        return carry

    with jax.named_scope("query_proj"):
        lax.fori_loop(0, rows // wide, query_block, 0)

    for source, target, device in ((rows, 0, after), (EDGE, EDGE + rows, before)):
        remote(
            p_ext.at[pl.ds(source, EDGE)], p_ext.at[pl.ds(target, EDGE)],
            sent.at[PH], got.at[PH], device,
        ).start()

    ring_advance(1, (0,))
    with jax.named_scope("w2_wait"):
        for k in (1, 3, 2):
            landed(part_at(c, b, 4 - k), x_sem.at[k])
            ring_start(4 - k)

    with jax.named_scope("kv2_wait"):
        landed(kvbuf.at[c, pl.ds(0, RING - 1)], got.at[KV2])
    remote(kvbuf.at[c], kvbuf.at[c], sent.at[KVD], got.at[KVD], (s, other)).start()

    with jax.named_scope("pool_halo"):
        landed(p_ext.at[pl.ds(0, 2 * EDGE)], got.at[PH])

    @pl.when(s == 0)
    def _():
        p_ext[pl.ds(0, EDGE), :] = jnp.zeros((EDGE, 2 * HEAD), BF16)

    @pl.when(s == n_sp - 1)
    def _():
        p_ext[pl.ds(EDGE + rows, EDGE), :] = jnp.zeros((EDGE, 2 * HEAD), BF16)

    reach = 1 + (t // 2 > 0) + 2 * (t // 2 > 1) + 4 * (t // 2 > 2)
    span = QB + 2 * EDGE
    apart = (
        lax.broadcasted_iota(jnp.int32, (QB, span), 1)
        - lax.broadcasted_iota(jnp.int32, (QB, span), 0) - EDGE
    )
    band = jnp.where((apart >= -reach) & (apart < reach), 1.0, 0.0).astype(BF16)
    row_id = lax.broadcasted_iota(jnp.int32, (QB, 1), 0)
    scales = jnp.concatenate([scale_v[...], scale_v[...]], axis=1)
    sinks = sink_v[...]

    def pool_block(i, carry):
        first = pl.multiple_of(i * QB, QB)
        sums = jnp.dot(band, p_ext[pl.ds(first, span), :], preferred_element_type=F32)
        position = row_id + (s * rows + first)
        counted = (
            jnp.minimum(position + reach, seq_total) - jnp.maximum(position - reach, 0)
        ).astype(F32)
        here = p_ext[pl.ds(pl.multiple_of(EDGE + first, EDGE), QB), :].astype(F32)
        pooled = (sums * (1.0 / counted) - here) * scales
        pool_v[pl.ds(first, QB), :] = swap_halves(pooled).astype(BF16)
        return carry

    with jax.named_scope("pool_mix"):
        lax.fori_loop(0, blocks, pool_block, 0, unroll=2)

    with jax.named_scope("kvd_wait"):
        landed(kvbuf.at[c], got.at[KVD])

    def join_rows(i, carry):
        for j in range(RING):
            at = pl.multiple_of((i * RING + j) * 2 * half_rows, 2 * half_rows)
            wkv[pl.ds(at, half_rows), :] = kvbuf[0, i, j]
            wkv[pl.ds(pl.multiple_of(at + half_rows, half_rows), half_rows), :] = kvbuf[1, j, i]
        return carry

    with jax.named_scope("kv_join"):
        lax.fori_loop(0, RING, join_rows, 0)

    def key_rows(first, count):
        at = pl.ds(pl.multiple_of(first, QB), count)
        value = jnp.dot(nrm[at, :], wkv[...], preferred_element_type=F32)
        kv_ext[pl.ds(pl.multiple_of(WINDOW + first, QB), count), :] = rotated(value, at).astype(BF16)

    with jax.named_scope("key_edge"):
        key_rows(0, QB)
        key_rows(rows - QB, QB)
    ring_advance(2, (0,))
    for source, target, device in ((rows, 0, after), (WINDOW, WINDOW + rows, before)):
        remote(
            kv_ext.at[pl.ds(source, WINDOW)], kv_ext.at[pl.ds(target, WINDOW)],
            sent.at[KH], got.at[KH], device,
        ).start()
    with jax.named_scope("key_rest"):
        key_rows(QB, wide)
        key_rows(QB + wide, wide)
    ring_advance(1, (1, 3, 2))
    with jax.named_scope("key_rest"):
        key_rows(QB + 2 * wide, wide)

    query_at = lax.broadcasted_iota(jnp.int32, (QB, QB), 0)
    key_at = lax.broadcasted_iota(jnp.int32, (QB, QB), 1)

    def attend(i):
        first = i * QB
        keys = kv_ext[pl.ds(first, QB + 2 * WINDOW), :]
        scores = lax.dot_general(
            q_v[pl.ds(first, QB), :], keys, (((1,), (1,)), ((), ())), preferred_element_type=F32
        )
        low_ok, high_ok = key_at >= query_at, key_at <= query_at
        if i == 0:
            low_ok = low_ok & (s > 0)
        if i == blocks - 1:
            high_ok = high_ok & (s < n_sp - 1)
        scores = jnp.concatenate(
            [
                jnp.where(low_ok, scores[:, :QB], NEG_BIG),
                scores[:, QB : 2 * QB],
                jnp.where(high_ok, scores[:, 2 * QB :], NEG_BIG),
            ],
            axis=1,
        )
        highest = jnp.maximum(jnp.max(scores, axis=-1, keepdims=True), sinks)
        expo = jnp.exp(scores - highest)
        total = jnp.sum(expo, axis=-1, keepdims=True) + jnp.exp(sinks - highest)
        weights = (expo * (1.0 / total)).astype(BF16)
        result = jnp.dot(weights, keys, preferred_element_type=F32)
        mix_send[i] = jnp.where(lane < HEAD, pool_v[pl.ds(first, QB), :].astype(F32), result).astype(BF16)

    def hand_over(i):
        @pl.when(i != t)
        def _():
            remote(mix_send.at[i], mix_recv.at[t], sent.at[MX], got.at[MX], (s, i)).start()

        @pl.when(i == t)
        def _():
            mix_recv[i] = mix_send[i]

    def attend_pair(i, j):
        with jax.named_scope("attend"):
            attend(i)
            attend(j)
        hand_over(i)
        hand_over(j)

    attend_pair(1, 2)
    ring_advance(3, (0,))
    attend_pair(3, 4)
    ring_advance(2, (1, 3, 2))
    attend_pair(5, 6)
    ring_advance(4, (0,))
    with jax.named_scope("key_halo"):
        landed(kv_ext.at[pl.ds(0, 2 * WINDOW)], got.at[KH])
    attend_pair(0, blocks - 1)
    ring_advance(3, (1, 3, 2))
    ring_advance(4, (1, 3, 2))

    with jax.named_scope("mix_wait"):
        landed(mix_recv.at[pl.ds(0, n_tp - 1)], got.at[MX])
    left, right = [], []
    for j in range(n_tp // 2):
        even, odd = mix_recv[2 * j].astype(F32), mix_recv[2 * j + 1].astype(F32)
        left.append(jnp.where(lane < HEAD, swap_halves(even), odd).astype(BF16))
        right.append(jnp.where(lane < HEAD, even, swap_halves(odd)).astype(BF16))
    mixed = jnp.concatenate(left + right, axis=1)

    with jax.named_scope("wd_wait"):
        landed(wbuf.at[c], got.at[WD])

    span_out = RING * width
    with jax.named_scope("out_proj"):
        for i in range(RING):
            parts = []
            for j in range(n_tp // 2):
                parts.append(wbuf[0, i, j].reshape(span_out, QB))
                parts.append(wbuf[1, :, j, i].reshape(span_out, QB))
            out[:, i * span_out : (i + 1) * span_out] = lax.dot_general(
                mixed, jnp.concatenate(parts, axis=1), (((1,), (1,)), ((), ())),
                preferred_element_type=F32,
            ).astype(BF16)

    with jax.named_scope("send_wait"):
        left_here(kvbuf.at[c, b, pl.ds(0, RING - 1)], sent.at[KV1])
        left_here(kvbuf.at[c, pl.ds(0, RING - 1)], sent.at[KV2])
        left_here(kvbuf.at[c], sent.at[KVD])
        left_here(wbuf.at[c, b, x, pl.ds(0, RING - 1)], sent.at[W1])
        left_here(wbuf.at[c, b, pl.ds(0, 3)], sent.at[W2])
        left_here(wbuf.at[c], sent.at[WD])
        left_here(wbuf.at[c, pl.ds(0, RING - 1), pl.ds(0, 2)], sent.at[RR])
        left_here(wbuf.at[c, pl.ds(0, RING - 1), pl.ds(0, 2)], sent.at[RL])
        left_here(p_ext.at[pl.ds(0, 2 * EDGE)], sent.at[PH])
        left_here(kv_ext.at[pl.ds(0, 2 * WINDOW)], sent.at[KH])
        left_here(mix_send.at[pl.ds(0, n_tp - 1)], sent.at[MX])


def body(tokens, norm_gain, w_query, w_key, w_value, w_pool_in, sink_logit, pool_scale, w_out):
    rows, features = tokens.shape
    n_sp, n_tp = lax.axis_size("sp"), lax.axis_size("tp")
    start, row = angle_tables(n_sp, rows)
    dma, vmem = pltpu.SemaphoreType.DMA, pltpu.VMEM
    half = w_key.shape[0] // 2
    width = w_out.shape[1]
    pair = 2 * HEAD
    scratch = [
        vmem((rows, features), BF16),
        vmem((rows, features), BF16),
        vmem((1, features), F32),
        vmem(w_key.shape, BF16),
        vmem(w_value.shape, BF16),
        vmem((1, HEAD), F32),
        vmem((1, 1), F32),
        vmem((8, pair), F32),
        vmem((2, rows, pair), F32),
        vmem((pair, features), BF16),
        vmem((2, RING, RING, half, pair), BF16),
        vmem((features, pair), BF16),
        vmem((2, RING, n_tp // 2, RING, width, w_out.shape[0]), BF16),
        vmem((rows, pair), BF16),
        vmem((rows + 2 * EDGE, pair), BF16),
        vmem((rows, pair), BF16),
        vmem((rows + 2 * WINDOW, pair), BF16),
        vmem((n_tp, QB, pair), BF16),
        vmem((n_tp, QB, pair), BF16),
        dma((10,)),
        dma((rows // QB,)),
        dma((11,)),
        dma((9,)),
        dma((4,)),
        dma((2, 16)),
    ]
    return pl.pallas_call(
        functools.partial(kernel, rows),
        name="mixer",
        out_shape=jax.ShapeDtypeStruct((rows // n_tp, w_out.shape[1] * n_sp), BF16),
        in_specs=[pl.BlockSpec(memory_space=pl.ANY)] * 11,
        out_specs=pl.BlockSpec(memory_space=pltpu.VMEM),
        scratch_shapes=scratch,
        compiler_params=pltpu.CompilerParams(
            collective_id=0, has_side_effects=True, vmem_limit_bytes=60 * 2**20
        ),
    )(
        tokens, norm_gain[None, :], w_query.T, w_key, w_value, w_pool_in.T, pool_scale[None, :], sink_logit[None, :], w_out.T,
        jnp.asarray(start), jnp.asarray(row),
    )


def solution(mesh):
    in_specs = (
        P("sp", None),
        P(),
        P(None, "tp"),
        P("sp", None),
        P("sp", None),
        P(None, "tp"),
        P("tp"),
        P("tp"),
        P("tp", "sp"),
    )
    out_specs = P(("sp", "tp"), None)
    return jax.shard_map(body, mesh=mesh, in_specs=in_specs, out_specs=out_specs, check_vma=False)
```

```python
import functools

import jax
import jax.numpy as jnp
import numpy as np
from jax import lax
from jax.experimental import pallas as pl
from jax.experimental.pallas import tpu as pltpu
from jax.sharding import PartitionSpec as P

HEAD = 64
WINDOW = 128
QB = 128
NEG_BIG = -1e30
EDGE = 16
RING = 8
ORDER = (1, 7, 2, 6, 3, 5, 4)
FAR_FIRST = (4, 5, 3, 6, 2, 7, 1)
MESH = pl.DeviceIdType.MESH
F32 = jnp.float32
BF16 = jnp.bfloat16


def angle_tables(n_sp, rows):
    half = HEAD // 2
    inverse = np.float32(10000.0) ** (-np.arange(half, dtype=np.float32) / np.float32(half))

    def pair(positions):
        angles = positions[:, None].astype(np.float64) * inverse[None, :].astype(np.float64)
        cosine, sine = np.cos(angles), np.sin(angles)
        ones = np.ones((len(positions), HEAD))
        c = np.concatenate([cosine, cosine, ones], axis=1)
        s = np.concatenate([-sine, sine, 0.0 * ones], axis=1)
        return c.astype(np.float32), s.astype(np.float32)

    def cut(value):
        scale = np.exp2(np.floor(np.log2(np.where(value == 0, 1.0, np.abs(value)))) - 7)
        return np.trunc(value / scale) * scale

    exact = inverse.astype(np.float64)
    pieces = [cut(exact)]
    pieces.append(cut(exact - pieces[0]))
    pieces.append(exact - pieces[0] - pieces[1])
    start = np.zeros((n_sp, 8, 2 * HEAD), np.float32)
    start[:, 0], start[:, 1] = pair(np.arange(n_sp) * rows)
    start[:, 2, :half], start[:, 2, half:HEAD] = -1.0, 1.0
    for row, value in zip(range(3, 7), (*pieces, exact)):
        start[:, row, :HEAD] = np.concatenate([value, value])
    return start, np.stack(pair(np.arange(rows)))


def kernel(
    rows,
    tokens,
    gain,
    w_query,
    w_key,
    w_value,
    w_pool,
    scale,
    sink,
    w_out,
    start_angles,
    row_angles,
    out,
    tok,
    nrm,
    gain_v,
    wk_v,
    wv_v,
    scale_v,
    sink_v,
    start_v,
    angles_v,
    wqp,
    kvbuf,
    wkv,
    wbuf,
    q_v,
    p_ext,
    pool_v,
    kv_ext,
    mix_send,
    mix_recv,
    out_v,
    load_sem,
    tok_sem,
    sent,
    got,
    x_sem,
    ring_sem,
    out_sem,
):
    s = lax.axis_index("sp")
    t = lax.axis_index("tp")
    n_sp = lax.axis_size("sp")
    n_tp = lax.axis_size("tp")
    x, c = t // 2, t % 2
    z, y = s // RING, s % RING
    a = y + c * (z - y)
    b = z + c * (y - z)
    features = tok.shape[1]
    blocks = rows // QB
    half_blocks = blocks // 2

    def load(src, dst, i):
        return pltpu.make_async_copy(src, dst, load_sem.at[i])

    early = [
        load(w_key, wk_v, 0), load(w_value, wv_v, 1), load(w_out, wbuf.at[c, b, x, a], 2),
    ]
    late = [
        load(gain, gain_v, 3),
        load(w_query, wqp.at[pl.ds(0, HEAD)], 4), load(w_pool, wqp.at[pl.ds(HEAD, HEAD)], 5),
        load(row_angles, angles_v, 6), load(start_angles.at[s], start_v, 7),
        load(scale, scale_v, 8), load(sink, sink_v, 9),
    ]
    tok_loads = [
        pltpu.make_async_copy(
            tokens.at[pl.ds(i * QB, QB)], tok.at[pl.ds(i * QB, QB)], tok_sem.at[i]
        )
        for i in range(blocks)
    ]
    step_a = 1 + (RING - 1) * c
    step_b = RING - (RING - 1) * c
    other = t + 1 - 2 * c

    def along_a(k):
        return (s + ((a + k) % RING - a) * step_a, t)

    def along_b(k):
        return (s + ((b + k) % RING - b) * step_b, t)

    def along_x(k):
        return (s, ((x + k) % 4) * 2 + c)

    def along_tp(k):
        return (s, (t + k) % n_tp)

    after = ((s + 1) % n_sp, t)
    before = ((s + n_sp - 1) % n_sp, t)

    barrier = pltpu.get_barrier_semaphore()
    far_peers = [along_a(k) for k in FAR_FIRST] + [along_b(k) for k in FAR_FIRST]
    near_peers = [along_tp(k) for k in range(1, n_tp)] + [after, before]

    def greet(devices):
        for peer in devices:
            pl.semaphore_signal(barrier, inc=1, device_id=peer, device_id_type=MESH)

    greet(far_peers)
    for copy in early:
        copy.start()
    greet(near_peers)

    def remote(src, dst, ssem, rsem, device):
        return pltpu.make_async_remote_copy(
            src_ref=src, dst_ref=dst, send_sem=ssem, recv_sem=rsem,
            device_id=device, device_id_type=MESH,
        )

    def landed(region, sem):
        remote(region, region, sem, sem, (s, other)).wait_recv()

    def left_here(region, sem):
        remote(region, region, sem, sem, (s, other)).wait_send()

    KV1, KV2, KVD, W1, W2, WD, PH, KH, MX, D4, X4, RR, RL, WL = range(14)

    with jax.named_scope("load_wait"):
        for copy in early:
            copy.wait()

    lane = lax.broadcasted_iota(jnp.int32, (1, 2 * HEAD), 1)

    def swap_halves(value):
        return pltpu.roll(value, HEAD, 1)

    wk_f, wv_f = wk_v[...].astype(F32), wv_v[...].astype(F32)
    low_head = t < n_tp // 2
    k_part = jnp.where(low_head, wk_f, swap_halves(wk_f))
    v_part = jnp.where(low_head, swap_halves(wv_f), wv_f)
    kv_piece = jnp.where(lane < HEAD, k_part, v_part)
    half_rows = kv_piece.shape[0] // 2
    kvbuf[c, b, a] = jnp.where(c == 0, kv_piece[:half_rows], kv_piece[half_rows:]).astype(BF16)
    width = wbuf.shape[4]

    for copy in (late[0], *tok_loads, *late[1:]):
        copy.start()

    with jax.named_scope("barrier_wait"):
        pl.semaphore_wait(barrier, len(far_peers) + len(near_peers))

    own_kv, own_w = kvbuf.at[c, b, a], wbuf.at[c, b, x, a]
    for k in FAR_FIRST:
        remote(own_kv, own_kv, sent.at[KV1], got.at[KV1], along_a(k)).start()
    for k in FAR_FIRST:
        remote(own_w, own_w, sent.at[W1], got.at[W1], along_a(k)).start()

    chunk, slab = 32, 128

    def slabs():
        return [slice(j * slab, (j + 1) * slab) for j in range(features // slab)]

    def norm_at(i):
        return pl.ds(pl.multiple_of(i * chunk, chunk), chunk)

    def norm_center(i):
        parts = [tok[norm_at(i), cols].astype(F32) for cols in slabs()]
        while len(parts) > 1:
            parts = [p + q for p, q in zip(parts[::2], parts[1::2])]
        return jnp.sum(parts[0], axis=-1, keepdims=True) * (1.0 / features)

    def norm_spread(i, center):
        total = [0.0, 0.0]
        for j, cols in enumerate(slabs()):
            shifted = tok[norm_at(i), cols].astype(F32) - center
            total[j % 2] = total[j % 2] + shifted * shifted
        spread = jnp.sum(total[0] + total[1], axis=-1, keepdims=True) * (1.0 / features)
        return lax.rsqrt(spread + 1e-06)

    def norm_store(i, center, inverse):
        for cols in slabs():
            shifted = tok[norm_at(i), cols].astype(F32) - center
            nrm[norm_at(i), cols] = (shifted * inverse * gain_v[:, cols]).astype(BF16)

    def norm_blocks(lo, hi):
        for i in range(lo, hi):
            tok_loads[i].wait()
        lo, hi = lo * QB // chunk, hi * QB // chunk

        def step(i, carry):
            later, center, inverse = carry
            norm_store(i, center, inverse)
            next_inverse = norm_spread(jnp.minimum(i + 1, hi - 1), later)
            return norm_center(jnp.minimum(i + 2, hi - 1)), later, next_inverse

        first = norm_center(lo)
        lax.fori_loop(lo, hi, step, (norm_center(lo + 1), first, norm_spread(lo, first)))

    late[0].wait()
    with jax.named_scope("norm_a"):
        norm_blocks(0, half_blocks)
    with jax.named_scope("norm_b"):
        norm_blocks(half_blocks, half_blocks + 2)
    with jax.named_scope("norm_c"):
        norm_blocks(half_blocks + 2, blocks)
    def rotated(value, at):
        partner = jnp.where(
            lane < HEAD // 2,
            pltpu.roll(value, 2 * HEAD - HEAD // 2, 1),
            pltpu.roll(value, HEAD // 2, 1),
        )
        return value * angles_v[0, at, :] + partner * angles_v[1, at, :]

    wide = 2 * QB
    query_scale = jnp.where(lane < HEAD, HEAD ** (-0.5), 0.0)

    def query_block(i, carry):
        at = pl.ds(pl.multiple_of(i * wide, wide), wide)
        value = lax.dot_general(
            nrm[at, :], wqp[...], (((1,), (1,)), ((), ())), preferred_element_type=F32
        )
        p_ext[pl.ds(pl.multiple_of(EDGE + i * wide, EDGE), wide), :] = value.astype(BF16)
        q_v[at, :] = (rotated(value, at) * query_scale).astype(BF16)
        return carry

    with jax.named_scope("kv1_wait"):
        landed(kvbuf.at[c, b, pl.ds(0, RING - 1)], got.at[KV1])
    line_kv = kvbuf.at[c, b]
    for k in FAR_FIRST:
        remote(line_kv, line_kv, sent.at[KV2], got.at[KV2], along_b(k)).start()
    with jax.named_scope("w1_wait"):
        landed(wbuf.at[c, b, x, pl.ds(0, RING - 1)], got.at[W1])

    def chunk_at(way, d):
        return (b + (RING - d if way == 0 else d)) % RING

    def part_at(owner, place, r):
        return wbuf.at[owner, place, (x + r) % 4]

    def ring_send(way, d, r):
        part = part_at(c, chunk_at(way, d), r)
        device = along_b(1 if way == 0 else RING - 1)
        remote(part, part, sent.at[RR + way], ring_sem.at[way, 4 * d + r], device).start()

    def cross(place, r, group=WD):
        part = part_at(c, place, r)
        remote(part, part, sent.at[group], got.at[group], (s, other)).start()

    def ring_start(r):
        ring_send(0, 0, r)
        ring_send(1, 0, r)
        cross(b, r)

    def ring_advance(d, parts):
        with jax.named_scope("ring_wait"):
            for r in parts:
                for way in range(2):
                    place = chunk_at(way, d)
                    landed(part_at(c, place, r), ring_sem.at[way, 4 * (d - 1) + r])
                    if d < 3:
                        ring_send(way, d, r)
                    cross(place, r, WL if d == 3 else WD)

    line_w = part_at(c, b, 0)
    for k in (2, 1, 3):
        remote(line_w, line_w, sent.at[W2], x_sem.at[k], along_x(k)).start()
    ring_start(0)
    remote(line_w, line_w, sent.at[D4], got.at[D4], along_b(4)).start()
    far = (b + 4) % RING

    def far_advance():
        with jax.named_scope("far_wait"):
            landed(part_at(c, far, 0), got.at[D4])
        for k in (2, 1, 3):
            part = part_at(c, far, 0)
            remote(part, part, sent.at[X4], got.at[X4], along_x(k)).start()
        cross(far, 0)

    def far_finish():
        with jax.named_scope("far_wait"):
            landed(wbuf.at[c, far, pl.ds(0, 3)], got.at[X4])
        for r in (1, 2, 3):
            cross(far, r)

    for copy in late[1:]:
        copy.wait()

    seq_total = n_sp * rows
    base_c, base_s = start_v[0:1, :], start_v[1:2, :]
    signed, piece_1, piece_2, piece_3, whole = (start_v[i : i + 1, :] for i in range(2, 7))
    turn_rows = 64

    def turn_block(i, carry):
        at = pl.ds(pl.multiple_of(i * turn_rows, turn_rows), turn_rows)
        row_c, row_s = angles_v[0, at, :], angles_v[1, at, :]
        cosine = base_c * row_c - base_s * row_s
        sine = base_s * row_c + base_c * row_s
        position = (
            lax.broadcasted_iota(jnp.int32, (turn_rows, 1), 0) + (s * rows + i * turn_rows)
        ).astype(F32)
        rounding = position * whole - position * piece_1
        rounding = rounding - position * piece_2 - position * piece_3
        rounding = rounding * signed
        angles_v[0, at, :] = cosine - rounding * sine
        angles_v[1, at, :] = sine + rounding * cosine
        return carry

    with jax.named_scope("turns"):
        lax.fori_loop(0, rows // turn_rows, turn_block, 0)

    with jax.named_scope("query_edge"):
        query_block(0, 0)
        query_block(rows // wide - 1, 0)
    for source, target, device in ((rows, 0, after), (EDGE, EDGE + rows, before)):
        remote(
            p_ext.at[pl.ds(source, EDGE)], p_ext.at[pl.ds(target, EDGE)],
            sent.at[PH], got.at[PH], device,
        ).start()
    with jax.named_scope("query_rest"):
        lax.fori_loop(1, rows // wide - 1, query_block, 0)

    with jax.named_scope("w2_wait"):
        for k in (1, 3, 2):
            landed(part_at(c, b, 4 - k), x_sem.at[k])
            ring_start(4 - k)

    with jax.named_scope("kv2_wait"):
        landed(kvbuf.at[c, pl.ds(0, RING - 1)], got.at[KV2])
    remote(kvbuf.at[c], kvbuf.at[c], sent.at[KVD], got.at[KVD], (s, other)).start()

    ring_advance(1, (0,))
    with jax.named_scope("pool_halo"):
        landed(p_ext.at[pl.ds(0, 2 * EDGE)], got.at[PH])

    @pl.when(s == 0)
    def _():
        p_ext[pl.ds(0, EDGE), :] = jnp.zeros((EDGE, 2 * HEAD), BF16)

    @pl.when(s == n_sp - 1)
    def _():
        p_ext[pl.ds(EDGE + rows, EDGE), :] = jnp.zeros((EDGE, 2 * HEAD), BF16)

    reach = 1 + (t // 2 > 0) + 2 * (t // 2 > 1) + 4 * (t // 2 > 2)
    span = QB + 2 * EDGE
    apart = (
        lax.broadcasted_iota(jnp.int32, (QB, span), 1)
        - lax.broadcasted_iota(jnp.int32, (QB, span), 0) - EDGE
    )
    band = jnp.where((apart >= -reach) & (apart < reach), 1.0, 0.0).astype(BF16)
    row_id = lax.broadcasted_iota(jnp.int32, (QB, 1), 0)
    scales = jnp.concatenate([scale_v[...], scale_v[...]], axis=1)
    sinks = jnp.broadcast_to(sink_v[...], (1, 2 * HEAD))

    def pool_block(i, carry):
        first = pl.multiple_of(i * QB, QB)
        sums = jnp.dot(band, p_ext[pl.ds(first, span), :], preferred_element_type=F32)
        position = row_id + (s * rows + first)
        counted = (
            jnp.minimum(position + reach, seq_total) - jnp.maximum(position - reach, 0)
        ).astype(F32)
        here = p_ext[pl.ds(pl.multiple_of(EDGE + first, EDGE), QB), :].astype(F32)
        pooled = (sums * (1.0 / counted) - here) * scales
        pool_v[pl.ds(first, QB), :] = swap_halves(pooled).astype(BF16)
        return carry

    with jax.named_scope("pool_mix"):
        lax.fori_loop(0, blocks, pool_block, 0, unroll=2)

    with jax.named_scope("kvd_wait"):
        landed(kvbuf.at[c], got.at[KVD])

    def join_rows(i, carry):
        for j in range(RING):
            at = pl.multiple_of((i * RING + j) * 2 * half_rows, 2 * half_rows)
            wkv[pl.ds(at, half_rows), :] = kvbuf[0, i, j]
            wkv[pl.ds(pl.multiple_of(at + half_rows, half_rows), half_rows), :] = kvbuf[1, j, i]
        return carry

    with jax.named_scope("kv_join"):
        lax.fori_loop(0, RING, join_rows, 0)

    def key_rows(first, count):
        at = pl.ds(pl.multiple_of(first, QB), count)
        value = jnp.dot(nrm[at, :], wkv[...], preferred_element_type=F32)
        kv_ext[pl.ds(pl.multiple_of(WINDOW + first, QB), count), :] = rotated(value, at).astype(BF16)

    with jax.named_scope("key_edge"):
        key_rows(0, QB)
        key_rows(rows - QB, QB)
    with jax.named_scope("key_rest"):
        key_rows(QB, wide)
    for source, target, device in ((rows, 0, after), (WINDOW, WINDOW + rows, before)):
        remote(
            kv_ext.at[pl.ds(source, WINDOW)], kv_ext.at[pl.ds(target, WINDOW)],
            sent.at[KH], got.at[KH], device,
        ).start()
    with jax.named_scope("key_rest"):
        key_rows(QB + wide, wide)
        key_rows(QB + 2 * wide, wide)

    query_at = lax.broadcasted_iota(jnp.int32, (QB, QB), 0)
    key_at = lax.broadcasted_iota(jnp.int32, (QB, QB), 1)

    def across_lanes(column):
        return jnp.broadcast_to(column, (QB, 2 * HEAD))

    def attend(blocks_now):
        window = [kv_ext[pl.ds(i * QB, QB + 2 * WINDOW), :] for i in blocks_now]
        scores = [
            lax.dot_general(
                q_v[pl.ds(i * QB, QB), :], keys, (((1,), (1,)), ((), ())),
                preferred_element_type=F32,
            )
            for i, keys in zip(blocks_now, window)
        ]
        tiles = []
        for i, score in zip(blocks_now, scores):
            low_ok, high_ok = key_at >= query_at, key_at <= query_at
            if i == 0:
                low_ok = low_ok & (s > 0)
            if i == blocks - 1:
                high_ok = high_ok & (s < n_sp - 1)
            tiles.append((
                jnp.where(low_ok, score[:, :QB], NEG_BIG),
                score[:, QB : 2 * QB],
                jnp.where(high_ok, score[:, 2 * QB :], NEG_BIG),
            ))
        highest = [
            jnp.max(jnp.maximum(jnp.maximum(p, q), r), axis=-1, keepdims=True) for p, q, r in tiles
        ]
        highest = [jnp.maximum(across_lanes(top), sinks) for top in highest]
        expo = [[jnp.exp(part - top) for part in three] for three, top in zip(tiles, highest)]
        total = [jnp.sum(p + q + r, axis=-1, keepdims=True) for p, q, r in expo]
        inverse = [
            1.0 / (across_lanes(some) + jnp.exp(sinks - top)) for some, top in zip(total, highest)
        ]
        weights = [
            jnp.concatenate([(part * one).astype(BF16) for part in three], axis=1)
            for three, one in zip(expo, inverse)
        ]
        result = [
            jnp.dot(some, keys, preferred_element_type=F32) for some, keys in zip(weights, window)
        ]
        for i, some in zip(blocks_now, result):
            mix_send[i] = jnp.where(
                lane < HEAD, pool_v[pl.ds(i * QB, QB), :].astype(F32), some
            ).astype(BF16)

    def hand_over(i):
        @pl.when(i != t)
        def _():
            remote(mix_send.at[i], mix_recv.at[t], sent.at[MX], got.at[MX], (s, i)).start()

        @pl.when(i == t)
        def _():
            mix_recv[i] = mix_send[i]

    def attend_pair(i, j):
        with jax.named_scope("attend"):
            attend((i, j))
        hand_over(i)
        hand_over(j)

    far_advance()
    ring_advance(1, (3,))
    attend_pair(1, 2)
    ring_advance(1, (1,))
    attend_pair(3, 4)
    ring_advance(1, (2,))
    attend_pair(5, 6)
    ring_advance(2, (0,))
    with jax.named_scope("key_halo"):
        landed(kv_ext.at[pl.ds(0, 2 * WINDOW)], got.at[KH])
    attend_pair(0, blocks - 1)
    ring_advance(2, (3,))
    ring_advance(2, (1,))
    ring_advance(2, (2,))
    far_finish()
    ring_advance(3, (0,))

    def group_region(owner, group):
        return wbuf.at[owner, pl.ds(0, 2 if group == WL else RING - 2)]

    def cross_wait(group):
        with jax.named_scope("cross_wait"):
            landed(group_region(1 - c, group), got.at[group])

    ring_advance(3, (3, 1, 2))
    cross_wait(WD)

    @pl.when(c == 0)
    def _():
        cross_wait(WL)

    left_here(kvbuf.at[c, b, pl.ds(0, RING - 1)], sent.at[KV1])
    with jax.named_scope("mix_wait"):
        landed(mix_recv.at[pl.ds(0, n_tp - 1)], got.at[MX])
    left, right = [], []
    for j in range(n_tp // 2):
        even, odd = mix_recv[2 * j].astype(F32), mix_recv[2 * j + 1].astype(F32)
        left.append(jnp.where(lane < HEAD, swap_halves(even), odd).astype(BF16))
        right.append(jnp.where(lane < HEAD, even, swap_halves(odd)).astype(BF16))
    mixed = jnp.concatenate(left + right, axis=1)

    span_out = RING * width
    stores = []

    def out_block(d):
        i = (z + d) % RING
        parts = []
        for j in range(n_tp // 2):
            parts.append(wbuf[0, i, j].reshape(span_out, QB))
            parts.append(wbuf[1, :, j, i].reshape(span_out, QB))
        cols = pl.ds(pl.multiple_of(i * span_out, span_out), span_out)
        out_v[:, cols] = lax.dot_general(
            mixed, jnp.concatenate(parts, axis=1), (((1,), (1,)), ((), ())),
            preferred_element_type=F32,
        ).astype(BF16)
        store = pltpu.make_async_copy(out_v.at[:, cols], out.at[:, cols], out_sem.at[d])
        store.start()
        stores.append(store)

    with jax.named_scope("out_most"):
        for d in (0, 1, 7, 2, 6, 4):
            out_block(d)

    @pl.when(c == 1)
    def _():
        cross_wait(WL)

    with jax.named_scope("out_last"):
        for d in (3, 5):
            out_block(d)

    with jax.named_scope("send_wait"):
        for store in stores:
            store.wait()
        left_here(kvbuf.at[c, pl.ds(0, RING - 1)], sent.at[KV2])
        left_here(kvbuf.at[c], sent.at[KVD])
        left_here(wbuf.at[c, b, x, pl.ds(0, RING - 1)], sent.at[W1])
        left_here(wbuf.at[c, b, pl.ds(0, 3)], sent.at[W2])
        left_here(group_region(c, WD), sent.at[WD])
        left_here(group_region(c, WL), sent.at[WL])
        left_here(part_at(c, b, 0), sent.at[D4])
        left_here(wbuf.at[c, far, pl.ds(0, 3)], sent.at[X4])
        left_here(wbuf.at[c, pl.ds(0, 3)], sent.at[RR])
        left_here(wbuf.at[c, pl.ds(0, 3)], sent.at[RL])
        left_here(p_ext.at[pl.ds(0, 2 * EDGE)], sent.at[PH])
        left_here(kv_ext.at[pl.ds(0, 2 * WINDOW)], sent.at[KH])
        left_here(mix_send.at[pl.ds(0, n_tp - 1)], sent.at[MX])


def body(tokens, norm_gain, w_query, w_key, w_value, w_pool_in, sink_logit, pool_scale, w_out):
    rows, features = tokens.shape
    n_sp, n_tp = lax.axis_size("sp"), lax.axis_size("tp")
    start, row = angle_tables(n_sp, rows)
    dma, vmem = pltpu.SemaphoreType.DMA, pltpu.VMEM
    half = w_key.shape[0] // 2
    width = w_out.shape[1]
    pair = 2 * HEAD
    scratch = [
        vmem((rows, features), BF16),
        vmem((rows, features), BF16),
        vmem((1, features), F32),
        vmem(w_key.shape, BF16),
        vmem(w_value.shape, BF16),
        vmem((1, HEAD), F32),
        vmem((1, 1), F32),
        vmem((8, pair), F32),
        vmem((2, rows, pair), F32),
        vmem((pair, features), BF16),
        vmem((2, RING, RING, half, pair), BF16),
        vmem((features, pair), BF16),
        vmem((2, RING, n_tp // 2, RING, width, w_out.shape[0]), BF16),
        vmem((rows, pair), BF16),
        vmem((rows + 2 * EDGE, pair), BF16),
        vmem((rows, pair), BF16),
        vmem((rows + 2 * WINDOW, pair), BF16),
        vmem((n_tp, QB, pair), BF16),
        vmem((n_tp, QB, pair), BF16),
        vmem((rows // n_tp, width * n_sp), BF16),
        dma((10,)),
        dma((rows // QB,)),
        dma((14,)),
        dma((14,)),
        dma((4,)),
        dma((2, 12)),
        dma((RING,)),
    ]
    return pl.pallas_call(
        functools.partial(kernel, rows),
        name="mixer",
        out_shape=jax.ShapeDtypeStruct((rows // n_tp, w_out.shape[1] * n_sp), BF16),
        in_specs=[pl.BlockSpec(memory_space=pl.ANY)] * 11,
        out_specs=pl.BlockSpec(memory_space=pl.ANY),
        scratch_shapes=scratch,
        compiler_params=pltpu.CompilerParams(
            collective_id=0, has_side_effects=True, vmem_limit_bytes=60 * 2**20
        ),
    )(
        tokens, norm_gain[None, :], w_query.T, w_key, w_value, w_pool_in.T, pool_scale[None, :], sink_logit[None, :], w_out.T,
        jnp.asarray(start), jnp.asarray(row),
    )


def solution(mesh):
    in_specs = (
        P("sp", None),
        P(),
        P(None, "tp"),
        P("sp", None),
        P("sp", None),
        P(None, "tp"),
        P("tp"),
        P("tp"),
        P("tp", "sp"),
    )
    out_specs = P(("sp", "tp"), None)
    return jax.shard_map(body, mesh=mesh, in_specs=in_specs, out_specs=out_specs, check_vma=False)
```

```python
import functools

import jax
import jax.numpy as jnp
import numpy as np
from jax import lax
from jax.experimental import pallas as pl
from jax.experimental.pallas import tpu as pltpu
from jax.sharding import PartitionSpec as P

HEAD = 64
WINDOW = 128
QB = 128
NEG_BIG = -1e30
EDGE = 16
RING = 8
ORDER = (1, 7, 2, 6, 3, 5, 4)
FAR_FIRST = (4, 5, 3, 6, 2, 7, 1)
MESH = pl.DeviceIdType.MESH
F32 = jnp.float32
BF16 = jnp.bfloat16


def angle_tables(n_sp, rows):
    half = HEAD // 2
    inverse = np.float32(10000.0) ** (-np.arange(half, dtype=np.float32) / np.float32(half))

    def pair(positions):
        angles = positions[:, None].astype(np.float64) * inverse[None, :].astype(np.float64)
        cosine, sine = np.cos(angles), np.sin(angles)
        ones = np.ones((len(positions), HEAD))
        c = np.concatenate([cosine, cosine, ones], axis=1)
        s = np.concatenate([-sine, sine, 0.0 * ones], axis=1)
        return c.astype(np.float32), s.astype(np.float32)

    def cut(value):
        scale = np.exp2(np.floor(np.log2(np.where(value == 0, 1.0, np.abs(value)))) - 7)
        return np.trunc(value / scale) * scale

    exact = inverse.astype(np.float64)
    pieces = [cut(exact)]
    pieces.append(cut(exact - pieces[0]))
    pieces.append(exact - pieces[0] - pieces[1])
    start = np.zeros((n_sp, 8, 2 * HEAD), np.float32)
    start[:, 0], start[:, 1] = pair(np.arange(n_sp) * rows)
    start[:, 2, :half], start[:, 2, half:HEAD] = -1.0, 1.0
    for row, value in zip(range(3, 7), (*pieces, exact)):
        start[:, row, :HEAD] = np.concatenate([value, value])
    return start, np.stack(pair(np.arange(rows)))


def kernel(
    rows,
    tokens,
    gain,
    w_query,
    w_key,
    w_value,
    w_pool,
    scale,
    sink,
    w_out,
    start_angles,
    row_angles,
    out,
    tok,
    nrm,
    gain_v,
    wk_v,
    wv_v,
    scale_v,
    sink_v,
    start_v,
    angles_v,
    wqp,
    kvbuf,
    wkv,
    wbuf,
    q_v,
    p_ext,
    pool_v,
    kv_ext,
    mix_send,
    mix_recv,
    out_v,
    load_sem,
    tok_sem,
    sent,
    got,
    x_sem,
    ring_sem,
    out_sem,
):
    s = lax.axis_index("sp")
    t = lax.axis_index("tp")
    n_sp = lax.axis_size("sp")
    n_tp = lax.axis_size("tp")
    x, c = t // 2, t % 2
    z, y = s // RING, s % RING
    a = y + c * (z - y)
    b = z + c * (y - z)
    features = tok.shape[1]
    blocks = rows // QB
    half_blocks = blocks // 2

    def load(src, dst, i):
        return pltpu.make_async_copy(src, dst, load_sem.at[i])

    early = [
        load(w_key, wk_v, 0), load(w_value, wv_v, 1), load(w_out, wbuf.at[c, b, x, a], 2),
    ]
    late = [
        load(gain, gain_v, 3),
        load(w_query, wqp.at[pl.ds(0, HEAD)], 4), load(w_pool, wqp.at[pl.ds(HEAD, HEAD)], 5),
        load(row_angles, angles_v, 6), load(start_angles.at[s], start_v, 7),
        load(scale, scale_v, 8), load(sink, sink_v, 9),
    ]
    tok_loads = [
        pltpu.make_async_copy(
            tokens.at[pl.ds(i * QB, QB)], tok.at[pl.ds(i * QB, QB)], tok_sem.at[i]
        )
        for i in range(blocks)
    ]
    step_a = 1 + (RING - 1) * c
    step_b = RING - (RING - 1) * c
    other = t + 1 - 2 * c

    def along_a(k):
        return (s + ((a + k) % RING - a) * step_a, t)

    def along_b(k):
        return (s + ((b + k) % RING - b) * step_b, t)

    def along_x(k):
        return (s, ((x + k) % 4) * 2 + c)

    def along_tp(k):
        return (s, (t + k) % n_tp)

    after = ((s + 1) % n_sp, t)
    before = ((s + n_sp - 1) % n_sp, t)

    barrier = pltpu.get_barrier_semaphore()
    far_peers = [along_a(k) for k in FAR_FIRST] + [along_b(k) for k in FAR_FIRST]
    near_peers = [along_tp(k) for k in range(1, n_tp)] + [after, before]
    for k in (1, RING - 1):
        near_peers += [(along_a(k)[0], other), (along_b(k)[0], other)]

    def greet(devices):
        for peer in devices:
            pl.semaphore_signal(barrier, inc=1, device_id=peer, device_id_type=MESH)

    greet(far_peers)
    for copy in early:
        copy.start()
    greet(near_peers)

    def remote(src, dst, ssem, rsem, device):
        return pltpu.make_async_remote_copy(
            src_ref=src, dst_ref=dst, send_sem=ssem, recv_sem=rsem,
            device_id=device, device_id_type=MESH,
        )

    def landed(region, sem):
        remote(region, region, sem, sem, (s, other)).wait_recv()

    def left_here(region, sem):
        remote(region, region, sem, sem, (s, other)).wait_send()

    KV1, KV2, KVD, W1, W2, WD, PH, KH, MX, D4, X4, RR, RL, WR, WL = range(15)

    with jax.named_scope("load_wait"):
        for copy in early:
            copy.wait()

    lane = lax.broadcasted_iota(jnp.int32, (1, 2 * HEAD), 1)

    def swap_halves(value):
        return pltpu.roll(value, HEAD, 1)

    wk_f, wv_f = wk_v[...].astype(F32), wv_v[...].astype(F32)
    low_head = t < n_tp // 2
    k_part = jnp.where(low_head, wk_f, swap_halves(wk_f))
    v_part = jnp.where(low_head, swap_halves(wv_f), wv_f)
    kv_piece = jnp.where(lane < HEAD, k_part, v_part)
    half_rows = kv_piece.shape[0] // 2
    kvbuf[c, b, a] = jnp.where(c == 0, kv_piece[:half_rows], kv_piece[half_rows:]).astype(BF16)
    width = wbuf.shape[4]

    for copy in (late[0], *tok_loads, *late[1:]):
        copy.start()

    with jax.named_scope("barrier_wait"):
        pl.semaphore_wait(barrier, len(far_peers) + len(near_peers))

    own_kv, own_w = kvbuf.at[c, b, a], wbuf.at[c, b, x, a]
    for k in FAR_FIRST:
        remote(own_w, own_w, sent.at[W1], got.at[W1], along_a(k)).start()
    for k in FAR_FIRST:
        remote(own_kv, own_kv, sent.at[KV1], got.at[KV1], along_a(k)).start()

    chunk, slab = 32, 128

    def slabs():
        return [slice(j * slab, (j + 1) * slab) for j in range(features // slab)]

    def norm_at(i):
        return pl.ds(pl.multiple_of(i * chunk, chunk), chunk)

    def norm_center(i):
        parts = [tok[norm_at(i), cols].astype(F32) for cols in slabs()]
        while len(parts) > 1:
            parts = [p + q for p, q in zip(parts[::2], parts[1::2])]
        return jnp.sum(parts[0], axis=-1, keepdims=True) * (1.0 / features)

    def norm_spread(i, center):
        total = [0.0, 0.0]
        for j, cols in enumerate(slabs()):
            shifted = tok[norm_at(i), cols].astype(F32) - center
            total[j % 2] = total[j % 2] + shifted * shifted
        spread = jnp.sum(total[0] + total[1], axis=-1, keepdims=True) * (1.0 / features)
        return lax.rsqrt(spread + 1e-06)

    def norm_store(i, center, inverse):
        for cols in slabs():
            shifted = tok[norm_at(i), cols].astype(F32) - center
            nrm[norm_at(i), cols] = (shifted * inverse * gain_v[:, cols]).astype(BF16)

    def norm_blocks(lo, hi):
        for i in range(lo, hi):
            tok_loads[i].wait()
        lo, hi = lo * QB // chunk, hi * QB // chunk

        def step(i, carry):
            later, center, inverse = carry
            norm_store(i, center, inverse)
            next_inverse = norm_spread(jnp.minimum(i + 1, hi - 1), later)
            return norm_center(jnp.minimum(i + 2, hi - 1)), later, next_inverse

        first = norm_center(lo)
        lax.fori_loop(lo, hi, step, (norm_center(lo + 1), first, norm_spread(lo, first)))

    late[0].wait()
    with jax.named_scope("norm_a"):
        norm_blocks(0, half_blocks)
    with jax.named_scope("norm_b"):
        norm_blocks(half_blocks, half_blocks + 2)
    with jax.named_scope("norm_c"):
        norm_blocks(half_blocks + 2, blocks)
    def rotated(value, at):
        partner = jnp.where(
            lane < HEAD // 2,
            pltpu.roll(value, 2 * HEAD - HEAD // 2, 1),
            pltpu.roll(value, HEAD // 2, 1),
        )
        return value * angles_v[0, at, :] + partner * angles_v[1, at, :]

    wide = 2 * QB
    query_scale = jnp.where(lane < HEAD, HEAD ** (-0.5), 0.0)

    def query_block(i, carry):
        at = pl.ds(pl.multiple_of(i * wide, wide), wide)
        value = lax.dot_general(
            nrm[at, :], wqp[...], (((1,), (1,)), ((), ())), preferred_element_type=F32
        )
        p_ext[pl.ds(pl.multiple_of(EDGE + i * wide, EDGE), wide), :] = value.astype(BF16)
        q_v[at, :] = (rotated(value, at) * query_scale).astype(BF16)
        return carry

    with jax.named_scope("w1_wait"):
        landed(wbuf.at[c, b, x, pl.ds(0, RING - 1)], got.at[W1])

    def chunk_at(way, d):
        return (b + (RING - d if way == 0 else d)) % RING

    def part_at(owner, place, r):
        return wbuf.at[owner, place, (x + r) % 4]

    def ring_send(way, d, r):
        part = part_at(c, chunk_at(way, d), r)
        device = along_b(1 if way == 0 else RING - 1)
        remote(part, part, sent.at[RR + way], ring_sem.at[way, 4 * d + r], device).start()

    def cross(place, r, group=WD):
        part = part_at(c, place, r)
        remote(part, part, sent.at[group], got.at[group], (s, other)).start()

    def ring_start(r):
        ring_send(0, 0, r)
        ring_send(1, 0, r)
        cross(b, r)

    def ring_event(d, r, way):
        place = chunk_at(way, d)
        part = part_at(c, place, r)
        landed(part, ring_sem.at[way, 4 * (d - 1) + r])
        last = (WR, WL)[way]
        if d < 3:
            ring_send(way, d, r)
        if d == 2 and r == 2:
            beside = (along_b(1 if way == 0 else RING - 1)[0], other)
            remote(part, part, sent.at[last], got.at[last], beside).start()
        if d < 3:
            cross(place, r)
        elif r != 2:
            cross(place, r, last)

    def ring_advance(d, parts):
        events = [(r, way) for r in parts for way in range(2)]
        if d == 3:
            events = [(r, way) for way in (1, 0) for r in parts]
        with jax.named_scope("ring_wait"):
            for r, way in events:
                ring_event(d, r, way)

    line_w = part_at(c, b, 0)
    for k in (2, 1, 3):
        remote(line_w, line_w, sent.at[W2], x_sem.at[k], along_x(k)).start()
    with jax.named_scope("kv1_wait"):
        landed(kvbuf.at[c, b, pl.ds(0, RING - 1)], got.at[KV1])
    line_kv = kvbuf.at[c, b]
    for k in FAR_FIRST:
        remote(line_kv, line_kv, sent.at[KV2], got.at[KV2], along_b(k)).start()
    ring_start(0)
    remote(line_w, line_w, sent.at[D4], got.at[D4], along_b(4)).start()
    far = (b + 4) % RING

    def far_advance():
        with jax.named_scope("far_wait"):
            landed(part_at(c, far, 0), got.at[D4])
        for k in (2, 1, 3):
            part = part_at(c, far, 0)
            remote(part, part, sent.at[X4], got.at[X4], along_x(k)).start()
        cross(far, 0)

    def far_finish():
        with jax.named_scope("far_wait"):
            landed(wbuf.at[c, far, pl.ds(0, 3)], got.at[X4])
        for r in (1, 2, 3):
            cross(far, r)

    for copy in late[1:]:
        copy.wait()

    seq_total = n_sp * rows
    base_c, base_s = start_v[0:1, :], start_v[1:2, :]
    signed, piece_1, piece_2, piece_3, whole = (start_v[i : i + 1, :] for i in range(2, 7))
    turn_rows = 64

    def turn_block(i, carry):
        at = pl.ds(pl.multiple_of(i * turn_rows, turn_rows), turn_rows)
        row_c, row_s = angles_v[0, at, :], angles_v[1, at, :]
        cosine = base_c * row_c - base_s * row_s
        sine = base_s * row_c + base_c * row_s
        position = (
            lax.broadcasted_iota(jnp.int32, (turn_rows, 1), 0) + (s * rows + i * turn_rows)
        ).astype(F32)
        rounding = position * whole - position * piece_1
        rounding = rounding - position * piece_2 - position * piece_3
        rounding = rounding * signed
        angles_v[0, at, :] = cosine - rounding * sine
        angles_v[1, at, :] = sine + rounding * cosine
        return carry

    with jax.named_scope("turns"):
        lax.fori_loop(0, rows // turn_rows, turn_block, 0)

    with jax.named_scope("query_edge"):
        query_block(0, 0)
        query_block(rows // wide - 1, 0)
    for source, target, device in ((rows, 0, after), (EDGE, EDGE + rows, before)):
        remote(
            p_ext.at[pl.ds(source, EDGE)], p_ext.at[pl.ds(target, EDGE)],
            sent.at[PH], got.at[PH], device,
        ).start()
    with jax.named_scope("query_rest"):
        lax.fori_loop(1, rows // wide - 1, query_block, 0)

    with jax.named_scope("w2_wait"):
        for k in (1, 3, 2):
            landed(part_at(c, b, 4 - k), x_sem.at[k])
            ring_start(4 - k)

    with jax.named_scope("kv2_wait"):
        landed(kvbuf.at[c, pl.ds(0, RING - 1)], got.at[KV2])
    remote(kvbuf.at[c], kvbuf.at[c], sent.at[KVD], got.at[KVD], (s, other)).start()

    ring_advance(1, (0,))
    with jax.named_scope("pool_halo"):
        landed(p_ext.at[pl.ds(0, 2 * EDGE)], got.at[PH])

    @pl.when(s == 0)
    def _():
        p_ext[pl.ds(0, EDGE), :] = jnp.zeros((EDGE, 2 * HEAD), BF16)

    @pl.when(s == n_sp - 1)
    def _():
        p_ext[pl.ds(EDGE + rows, EDGE), :] = jnp.zeros((EDGE, 2 * HEAD), BF16)

    reach = 1 + (t // 2 > 0) + 2 * (t // 2 > 1) + 4 * (t // 2 > 2)
    span = QB + 2 * EDGE
    apart = (
        lax.broadcasted_iota(jnp.int32, (QB, span), 1)
        - lax.broadcasted_iota(jnp.int32, (QB, span), 0) - EDGE
    )
    band = jnp.where((apart >= -reach) & (apart < reach), 1.0, 0.0).astype(BF16)
    row_id = lax.broadcasted_iota(jnp.int32, (QB, 1), 0)
    scales = jnp.concatenate([scale_v[...], scale_v[...]], axis=1)
    sinks = jnp.broadcast_to(sink_v[...], (1, 2 * HEAD))

    def pool_block(i, carry):
        first = pl.multiple_of(i * QB, QB)
        sums = jnp.dot(band, p_ext[pl.ds(first, span), :], preferred_element_type=F32)
        position = row_id + (s * rows + first)
        counted = (
            jnp.minimum(position + reach, seq_total) - jnp.maximum(position - reach, 0)
        ).astype(F32)
        here = p_ext[pl.ds(pl.multiple_of(EDGE + first, EDGE), QB), :].astype(F32)
        pooled = (sums * (1.0 / counted) - here) * scales
        pool_v[pl.ds(first, QB), :] = swap_halves(pooled).astype(BF16)
        return carry

    with jax.named_scope("pool_mix"):
        lax.fori_loop(0, blocks, pool_block, 0, unroll=2)

    with jax.named_scope("kvd_wait"):
        landed(kvbuf.at[c], got.at[KVD])

    def join_rows(i, carry):
        for j in range(RING):
            at = pl.multiple_of((i * RING + j) * 2 * half_rows, 2 * half_rows)
            wkv[pl.ds(at, half_rows), :] = kvbuf[0, i, j]
            wkv[pl.ds(pl.multiple_of(at + half_rows, half_rows), half_rows), :] = kvbuf[1, j, i]
        return carry

    with jax.named_scope("kv_join"):
        lax.fori_loop(0, RING, join_rows, 0)

    def key_rows(first, count):
        at = pl.ds(pl.multiple_of(first, QB), count)
        value = jnp.dot(nrm[at, :], wkv[...], preferred_element_type=F32)
        kv_ext[pl.ds(pl.multiple_of(WINDOW + first, QB), count), :] = rotated(value, at).astype(BF16)

    with jax.named_scope("key_edge"):
        key_rows(0, QB)
        key_rows(rows - QB, QB)
    ring_advance(1, (3,))
    with jax.named_scope("key_rest"):
        key_rows(QB, wide)
    for source, target, device in ((rows, 0, after), (WINDOW, WINDOW + rows, before)):
        remote(
            kv_ext.at[pl.ds(source, WINDOW)], kv_ext.at[pl.ds(target, WINDOW)],
            sent.at[KH], got.at[KH], device,
        ).start()
    far_advance()
    ring_advance(1, (1,))
    with jax.named_scope("key_rest"):
        key_rows(QB + wide, wide)
    ring_advance(1, (2,))
    with jax.named_scope("key_rest"):
        key_rows(QB + 2 * wide, wide)

    query_at = lax.broadcasted_iota(jnp.int32, (QB, QB), 0)
    key_at = lax.broadcasted_iota(jnp.int32, (QB, QB), 1)

    def across_lanes(column):
        return jnp.broadcast_to(column, (QB, 2 * HEAD))

    def attend(blocks_now):
        window = [kv_ext[pl.ds(i * QB, QB + 2 * WINDOW), :] for i in blocks_now]
        scores = [
            lax.dot_general(
                q_v[pl.ds(i * QB, QB), :], keys, (((1,), (1,)), ((), ())),
                preferred_element_type=F32,
            )
            for i, keys in zip(blocks_now, window)
        ]
        tiles = []
        for i, score in zip(blocks_now, scores):
            low_ok, high_ok = key_at >= query_at, key_at <= query_at
            if i == 0:
                low_ok = low_ok & (s > 0)
            if i == blocks - 1:
                high_ok = high_ok & (s < n_sp - 1)
            tiles.append((
                jnp.where(low_ok, score[:, :QB], NEG_BIG),
                score[:, QB : 2 * QB],
                jnp.where(high_ok, score[:, 2 * QB :], NEG_BIG),
            ))
        highest = [
            jnp.max(jnp.maximum(jnp.maximum(p, q), r), axis=-1, keepdims=True) for p, q, r in tiles
        ]
        highest = [jnp.maximum(across_lanes(top), sinks) for top in highest]
        expo = [[jnp.exp(part - top) for part in three] for three, top in zip(tiles, highest)]
        total = [jnp.sum(p + q + r, axis=-1, keepdims=True) for p, q, r in expo]
        inverse = [
            1.0 / (across_lanes(some) + jnp.exp(sinks - top)) for some, top in zip(total, highest)
        ]
        weights = [
            jnp.concatenate([(part * one).astype(BF16) for part in three], axis=1)
            for three, one in zip(expo, inverse)
        ]
        result = [
            jnp.dot(some, keys, preferred_element_type=F32) for some, keys in zip(weights, window)
        ]
        for i, some in zip(blocks_now, result):
            mix_send[i] = jnp.where(
                lane < HEAD, pool_v[pl.ds(i * QB, QB), :].astype(F32), some
            ).astype(BF16)

    def hand_over(i):
        @pl.when(i != t)
        def _():
            remote(mix_send.at[i], mix_recv.at[t], sent.at[MX], got.at[MX], (s, i)).start()

        @pl.when(i == t)
        def _():
            mix_recv[i] = mix_send[i]

    def attend_pair(i, j):
        with jax.named_scope("attend"):
            attend((i, j))
        hand_over(i)
        hand_over(j)

    attend_pair(1, 2)
    attend_pair(3, 4)
    ring_advance(2, (0,))
    attend_pair(5, 6)
    ring_advance(2, (3,))
    with jax.named_scope("key_halo"):
        landed(kv_ext.at[pl.ds(0, 2 * WINDOW)], got.at[KH])
    attend_pair(0, blocks - 1)
    ring_advance(2, (1,))
    ring_advance(2, (2,))
    far_finish()

    def group_region(owner, group):
        return wbuf.at[owner, pl.ds(0, RING - 2 if group == WD else 1)]

    def cross_wait(group):
        with jax.named_scope("cross_wait"):
            landed(group_region(1 - c, group), got.at[group])

    ring_advance(3, (0, 3, 1, 2))
    cross_wait(WD)

    @pl.when(c == 0)
    def _():
        cross_wait(WL)
        cross_wait(WR)

    left_here(kvbuf.at[c, b, pl.ds(0, RING - 1)], sent.at[KV1])
    with jax.named_scope("mix_wait"):
        landed(mix_recv.at[pl.ds(0, n_tp - 1)], got.at[MX])
    left, right = [], []
    for j in range(n_tp // 2):
        even, odd = mix_recv[2 * j].astype(F32), mix_recv[2 * j + 1].astype(F32)
        left.append(jnp.where(lane < HEAD, swap_halves(even), odd).astype(BF16))
        right.append(jnp.where(lane < HEAD, even, swap_halves(odd)).astype(BF16))
    mixed = jnp.concatenate(left + right, axis=1)

    span_out = RING * width

    def out_block(d):
        i = (z + d) % RING
        parts = []
        for j in range(n_tp // 2):
            parts.append(wbuf[0, i, j].reshape(span_out, QB))
            parts.append(wbuf[1, :, j, i].reshape(span_out, QB))
        cols = pl.ds(pl.multiple_of(i * span_out, span_out), span_out)
        out_v[:, cols] = lax.dot_general(
            mixed, jnp.concatenate(parts, axis=1), (((1,), (1,)), ((), ())),
            preferred_element_type=F32,
        ).astype(BF16)
        store = pltpu.make_async_copy(out_v.at[:, cols], out.at[:, cols], out_sem.at[0])
        store.start()

    with jax.named_scope("out_most"):
        for d in (0, 1, 7, 2, 6, 4):
            out_block(d)

    for d, group in ((3, WL), (5, WR)):
        @pl.when(c == 1)
        def _():
            cross_wait(group)

        with jax.named_scope("out_last"):
            out_block(d)

    with jax.named_scope("send_wait"):
        pltpu.make_async_copy(out_v, out, out_sem.at[0]).wait()
        left_here(kvbuf.at[c, pl.ds(0, RING - 1)], sent.at[KV2])
        left_here(kvbuf.at[c], sent.at[KVD])
        left_here(wbuf.at[c, b, x, pl.ds(0, RING - 1)], sent.at[W1])
        left_here(wbuf.at[c, b, pl.ds(0, 3)], sent.at[W2])
        left_here(group_region(c, WD), sent.at[WD])
        left_here(group_region(c, WL), sent.at[WL])
        left_here(group_region(c, WR), sent.at[WR])
        left_here(part_at(c, b, 0), sent.at[D4])
        left_here(wbuf.at[c, far, pl.ds(0, 3)], sent.at[X4])
        left_here(wbuf.at[c, pl.ds(0, 3)], sent.at[RR])
        left_here(wbuf.at[c, pl.ds(0, 3)], sent.at[RL])
        left_here(p_ext.at[pl.ds(0, 2 * EDGE)], sent.at[PH])
        left_here(kv_ext.at[pl.ds(0, 2 * WINDOW)], sent.at[KH])
        left_here(mix_send.at[pl.ds(0, n_tp - 1)], sent.at[MX])


def body(tokens, norm_gain, w_query, w_key, w_value, w_pool_in, sink_logit, pool_scale, w_out):
    rows, features = tokens.shape
    n_sp, n_tp = lax.axis_size("sp"), lax.axis_size("tp")
    start, row = angle_tables(n_sp, rows)
    dma, vmem = pltpu.SemaphoreType.DMA, pltpu.VMEM
    half = w_key.shape[0] // 2
    width = w_out.shape[1]
    pair = 2 * HEAD
    scratch = [
        vmem((rows, features), BF16),
        vmem((rows, features), BF16),
        vmem((1, features), F32),
        vmem(w_key.shape, BF16),
        vmem(w_value.shape, BF16),
        vmem((1, HEAD), F32),
        vmem((1, 1), F32),
        vmem((8, pair), F32),
        vmem((2, rows, pair), F32),
        vmem((pair, features), BF16),
        vmem((2, RING, RING, half, pair), BF16),
        vmem((features, pair), BF16),
        vmem((2, RING, n_tp // 2, RING, width, w_out.shape[0]), BF16),
        vmem((rows, pair), BF16),
        vmem((rows + 2 * EDGE, pair), BF16),
        vmem((rows, pair), BF16),
        vmem((rows + 2 * WINDOW, pair), BF16),
        vmem((n_tp, QB, pair), BF16),
        vmem((n_tp, QB, pair), BF16),
        vmem((rows // n_tp, width * n_sp), BF16),
        dma((10,)),
        dma((rows // QB,)),
        dma((15,)),
        dma((15,)),
        dma((4,)),
        dma((2, 12)),
        dma((1,)),
    ]
    return pl.pallas_call(
        functools.partial(kernel, rows),
        name="mixer",
        out_shape=jax.ShapeDtypeStruct((rows // n_tp, w_out.shape[1] * n_sp), BF16),
        in_specs=[pl.BlockSpec(memory_space=pl.ANY)] * 11,
        out_specs=pl.BlockSpec(memory_space=pl.ANY),
        scratch_shapes=scratch,
        compiler_params=pltpu.CompilerParams(
            collective_id=0, has_side_effects=True, vmem_limit_bytes=60 * 2**20
        ),
    )(
        tokens, norm_gain[None, :], w_query.T, w_key, w_value, w_pool_in.T, pool_scale[None, :], sink_logit[None, :], w_out.T,
        jnp.asarray(start), jnp.asarray(row),
    )


def solution(mesh):
    in_specs = (
        P("sp", None),
        P(),
        P(None, "tp"),
        P("sp", None),
        P("sp", None),
        P(None, "tp"),
        P("tp"),
        P("tp"),
        P("tp", "sp"),
    )
    out_specs = P(("sp", "tp"), None)
    return jax.shard_map(body, mesh=mesh, in_specs=in_specs, out_specs=out_specs, check_vma=False)
```

```python
import functools

import jax
import jax.numpy as jnp
import numpy as np
from jax import lax
from jax.experimental import pallas as pl
from jax.experimental.pallas import tpu as pltpu
from jax.sharding import PartitionSpec as P

HEAD = 64
WINDOW = 128
QB = 128
NEG_BIG = -1e30
EDGE = 16
RING = 8
ORDER = (1, 7, 2, 6, 3, 5, 4)
FAR_FIRST = (4, 5, 3, 6, 2, 7, 1)
MESH = pl.DeviceIdType.MESH
F32 = jnp.float32
BF16 = jnp.bfloat16


def angle_tables(n_sp, rows):
    half = HEAD // 2
    inverse = np.float32(10000.0) ** (-np.arange(half, dtype=np.float32) / np.float32(half))

    def pair(positions):
        angles = positions[:, None].astype(np.float64) * inverse[None, :].astype(np.float64)
        cosine, sine = np.cos(angles), np.sin(angles)
        ones = np.ones((len(positions), HEAD))
        c = np.concatenate([cosine, cosine, ones], axis=1)
        s = np.concatenate([-sine, sine, 0.0 * ones], axis=1)
        return c.astype(np.float32), s.astype(np.float32)

    def cut(value):
        scale = np.exp2(np.floor(np.log2(np.where(value == 0, 1.0, np.abs(value)))) - 7)
        return np.trunc(value / scale) * scale

    exact = inverse.astype(np.float64)
    pieces = [cut(exact)]
    pieces.append(cut(exact - pieces[0]))
    pieces.append(exact - pieces[0] - pieces[1])
    start = np.zeros((n_sp, 8, 2 * HEAD), np.float32)
    start[:, 0], start[:, 1] = pair(np.arange(n_sp) * rows)
    start[:, 2, :half], start[:, 2, half:HEAD] = -1.0, 1.0
    for row, value in zip(range(3, 7), (*pieces, exact)):
        start[:, row, :HEAD] = np.concatenate([value, value])
    return start, np.stack(pair(np.arange(rows)))


def kernel(
    rows,
    tokens,
    gain,
    w_query,
    w_key,
    w_value,
    w_pool,
    scale,
    sink,
    w_out,
    start_angles,
    row_angles,
    out,
    tok,
    nrm,
    gain_v,
    wk_v,
    wv_v,
    scale_v,
    sink_v,
    start_v,
    angles_v,
    wqp,
    kvbuf,
    wkv,
    wbuf,
    q_v,
    p_ext,
    pool_v,
    kv_ext,
    mix_send,
    mix_recv,
    out_v,
    load_sem,
    tok_sem,
    sent,
    got,
    x_sem,
    ring_sem,
    out_sem,
):
    s = lax.axis_index("sp")
    t = lax.axis_index("tp")
    n_sp = lax.axis_size("sp")
    n_tp = lax.axis_size("tp")
    x, c = t // 2, t % 2
    z, y = s // RING, s % RING
    a = y + c * (z - y)
    b = z + c * (y - z)
    features = tok.shape[1]
    blocks = rows // QB
    half_blocks = blocks // 2

    def load(src, dst, i):
        return pltpu.make_async_copy(src, dst, load_sem.at[i])

    early = [
        load(w_key, wk_v, 0), load(w_value, wv_v, 1), load(w_out, wbuf.at[c, b, x, a], 2),
    ]
    late = [
        load(gain, gain_v, 3),
        load(w_query, wqp.at[pl.ds(0, HEAD)], 4), load(w_pool, wqp.at[pl.ds(HEAD, HEAD)], 5),
        load(row_angles, angles_v, 6), load(start_angles.at[s], start_v, 7),
        load(scale, scale_v, 8), load(sink, sink_v, 9),
    ]
    tok_loads = [
        pltpu.make_async_copy(
            tokens.at[pl.ds(i * QB, QB)], tok.at[pl.ds(i * QB, QB)], tok_sem.at[i]
        )
        for i in range(blocks)
    ]
    step_a = 1 + (RING - 1) * c
    step_b = RING - (RING - 1) * c
    other = t + 1 - 2 * c

    def along_a(k):
        return (s + ((a + k) % RING - a) * step_a, t)

    def along_b(k):
        return (s + ((b + k) % RING - b) * step_b, t)

    def along_x(k):
        return (s, ((x + k) % 4) * 2 + c)

    def along_tp(k):
        return (s, (t + k) % n_tp)

    after = ((s + 1) % n_sp, t)
    before = ((s + n_sp - 1) % n_sp, t)

    barrier = pltpu.get_barrier_semaphore()
    far_peers = [along_a(k) for k in FAR_FIRST] + [along_b(k) for k in FAR_FIRST]
    near_peers = [along_tp(k) for k in range(1, n_tp)] + [after, before]
    for k in (1, RING - 1):
        near_peers += [(along_a(k)[0], other), (along_b(k)[0], other)]

    def greet(devices):
        for peer in devices:
            pl.semaphore_signal(barrier, inc=1, device_id=peer, device_id_type=MESH)

    greet(far_peers)
    for copy in early:
        copy.start()
    greet(near_peers)

    def remote(src, dst, ssem, rsem, device):
        return pltpu.make_async_remote_copy(
            src_ref=src, dst_ref=dst, send_sem=ssem, recv_sem=rsem,
            device_id=device, device_id_type=MESH,
        )

    def landed(region, sem):
        remote(region, region, sem, sem, (s, other)).wait_recv()

    def left_here(region, sem):
        remote(region, region, sem, sem, (s, other)).wait_send()

    KV1, KV2, KVD, W1, W2, WD, PH, KH, MX, D4, X4, RR, RL, WR, WL = range(15)

    with jax.named_scope("load_wait"):
        for copy in early:
            copy.wait()

    lane = lax.broadcasted_iota(jnp.int32, (1, 2 * HEAD), 1)

    def swap_halves(value):
        return pltpu.roll(value, HEAD, 1)

    wk_f, wv_f = wk_v[...].astype(F32), wv_v[...].astype(F32)
    low_head = t < n_tp // 2
    k_part = jnp.where(low_head, wk_f, swap_halves(wk_f))
    v_part = jnp.where(low_head, swap_halves(wv_f), wv_f)
    kv_piece = jnp.where(lane < HEAD, k_part, v_part)
    half_rows = kv_piece.shape[0] // 2
    kvbuf[c, b, a] = jnp.where(c == 0, kv_piece[:half_rows], kv_piece[half_rows:]).astype(BF16)
    width = wbuf.shape[4]

    for copy in (late[0], *tok_loads, *late[1:]):
        copy.start()

    with jax.named_scope("barrier_wait"):
        pl.semaphore_wait(barrier, len(far_peers) + len(near_peers))

    own_kv, own_w = kvbuf.at[c, b, a], wbuf.at[c, b, x, a]
    for k in FAR_FIRST:
        remote(own_w, own_w, sent.at[W1], got.at[W1], along_a(k)).start()
    for k in FAR_FIRST:
        remote(own_kv, own_kv, sent.at[KV1], got.at[KV1], along_a(k)).start()

    chunk, slab = 32, 128

    def slabs():
        return [slice(j * slab, (j + 1) * slab) for j in range(features // slab)]

    def norm_at(i):
        return pl.ds(pl.multiple_of(i * chunk, chunk), chunk)

    def norm_center(i):
        parts = [tok[norm_at(i), cols].astype(F32) for cols in slabs()]
        while len(parts) > 1:
            parts = [p + q for p, q in zip(parts[::2], parts[1::2])]
        return jnp.sum(parts[0], axis=-1, keepdims=True) * (1.0 / features)

    def norm_spread(i, center):
        total = [0.0, 0.0]
        for j, cols in enumerate(slabs()):
            shifted = tok[norm_at(i), cols].astype(F32) - center
            total[j % 2] = total[j % 2] + shifted * shifted
        spread = jnp.sum(total[0] + total[1], axis=-1, keepdims=True) * (1.0 / features)
        return lax.rsqrt(spread + 1e-06)

    def norm_store(i, center, inverse):
        for cols in slabs():
            shifted = tok[norm_at(i), cols].astype(F32) - center
            nrm[norm_at(i), cols] = (shifted * inverse * gain_v[:, cols]).astype(BF16)

    def norm_blocks(lo, hi):
        for i in range(lo, hi):
            tok_loads[i].wait()
        lo, hi = lo * QB // chunk, hi * QB // chunk

        def step(i, carry):
            later, center, inverse = carry
            norm_store(i, center, inverse)
            next_inverse = norm_spread(jnp.minimum(i + 1, hi - 1), later)
            return norm_center(jnp.minimum(i + 2, hi - 1)), later, next_inverse

        first = norm_center(lo)
        lax.fori_loop(lo, hi, step, (norm_center(lo + 1), first, norm_spread(lo, first)))

    late[0].wait()
    with jax.named_scope("norm_a"):
        norm_blocks(0, half_blocks)
    with jax.named_scope("norm_b"):
        norm_blocks(half_blocks, half_blocks + 2)
    with jax.named_scope("norm_c"):
        norm_blocks(half_blocks + 2, blocks)
    def rotated(value, at):
        partner = jnp.where(
            lane < HEAD // 2,
            pltpu.roll(value, 2 * HEAD - HEAD // 2, 1),
            pltpu.roll(value, HEAD // 2, 1),
        )
        return value * angles_v[0, at, :] + partner * angles_v[1, at, :]

    wide = 2 * QB
    query_scale = jnp.where(lane < HEAD, HEAD ** (-0.5), 0.0)

    def query_block(i, carry):
        at = pl.ds(pl.multiple_of(i * wide, wide), wide)
        value = lax.dot_general(
            nrm[at, :], wqp[...], (((1,), (1,)), ((), ())), preferred_element_type=F32
        )
        p_ext[pl.ds(pl.multiple_of(EDGE + i * wide, EDGE), wide), :] = value.astype(BF16)
        q_v[at, :] = (rotated(value, at) * query_scale).astype(BF16)
        return carry

    with jax.named_scope("w1_wait"):
        landed(wbuf.at[c, b, x, pl.ds(0, RING - 1)], got.at[W1])

    def chunk_at(way, d):
        return (b + (RING - d if way == 0 else d)) % RING

    def part_at(owner, place, r):
        return wbuf.at[owner, place, (x + r) % 4]

    def ring_send(way, d, r):
        part = part_at(c, chunk_at(way, d), r)
        device = along_b(1 if way == 0 else RING - 1)
        remote(part, part, sent.at[RR + way], ring_sem.at[way, 4 * d + r], device).start()

    def cross(place, r, group=WD):
        part = part_at(c, place, r)
        remote(part, part, sent.at[group], got.at[group], (s, other)).start()

    def ring_start(r):
        ring_send(0, 0, r)
        ring_send(1, 0, r)
        cross(b, r)

    def ring_event(d, r, way):
        place = chunk_at(way, d)
        part = part_at(c, place, r)
        landed(part, ring_sem.at[way, 4 * (d - 1) + r])
        last = (WR, WL)[way]
        if d < 3:
            ring_send(way, d, r)
        if d == 2 and r == 2:
            beside = (along_b(1 if way == 0 else RING - 1)[0], other)
            remote(part, part, sent.at[last], got.at[last], beside).start()
        if d < 3:
            cross(place, r)
        elif r != 2:
            cross(place, r, last)

    def ring_advance(d, parts):
        events = [(r, way) for r in parts for way in range(2)]
        if d == 3:
            events = [(r, way) for way in (1, 0) for r in parts]
        with jax.named_scope("ring_wait"):
            for r, way in events:
                ring_event(d, r, way)

    line_w = part_at(c, b, 0)
    for k in (2, 1, 3):
        remote(line_w, line_w, sent.at[W2], x_sem.at[k], along_x(k)).start()
    with jax.named_scope("kv1_wait"):
        landed(kvbuf.at[c, b, pl.ds(0, RING - 1)], got.at[KV1])
    line_kv = kvbuf.at[c, b]
    for k in FAR_FIRST:
        remote(line_kv, line_kv, sent.at[KV2], got.at[KV2], along_b(k)).start()
    ring_start(0)
    remote(line_w, line_w, sent.at[D4], got.at[D4], along_b(4)).start()
    far = (b + 4) % RING

    def far_advance():
        with jax.named_scope("far_wait"):
            landed(part_at(c, far, 0), got.at[D4])
        for k in (2, 1, 3):
            part = part_at(c, far, 0)
            remote(part, part, sent.at[X4], got.at[X4], along_x(k)).start()
        cross(far, 0)

    def far_finish():
        with jax.named_scope("far_wait"):
            landed(wbuf.at[c, far, pl.ds(0, 3)], got.at[X4])
        for r in (1, 2, 3):
            cross(far, r)

    for copy in late[1:]:
        copy.wait()

    seq_total = n_sp * rows
    base_c, base_s = start_v[0:1, :], start_v[1:2, :]
    signed, piece_1, piece_2, piece_3, whole = (start_v[i : i + 1, :] for i in range(2, 7))
    turn_rows = 64

    def turn_block(i, carry):
        at = pl.ds(pl.multiple_of(i * turn_rows, turn_rows), turn_rows)
        row_c, row_s = angles_v[0, at, :], angles_v[1, at, :]
        cosine = base_c * row_c - base_s * row_s
        sine = base_s * row_c + base_c * row_s
        position = (
            lax.broadcasted_iota(jnp.int32, (turn_rows, 1), 0) + (s * rows + i * turn_rows)
        ).astype(F32)
        rounding = position * whole - position * piece_1
        rounding = rounding - position * piece_2 - position * piece_3
        rounding = rounding * signed
        angles_v[0, at, :] = cosine - rounding * sine
        angles_v[1, at, :] = sine + rounding * cosine
        return carry

    with jax.named_scope("turns"):
        lax.fori_loop(0, rows // turn_rows, turn_block, 0)

    with jax.named_scope("query_edge"):
        query_block(0, 0)
        query_block(rows // wide - 1, 0)
    for source, target, device in ((rows, 0, after), (EDGE, EDGE + rows, before)):
        remote(
            p_ext.at[pl.ds(source, EDGE)], p_ext.at[pl.ds(target, EDGE)],
            sent.at[PH], got.at[PH], device,
        ).start()
    with jax.named_scope("query_rest"):
        lax.fori_loop(1, rows // wide - 1, query_block, 0)

    with jax.named_scope("w2_wait"):
        for k in (1, 3, 2):
            landed(part_at(c, b, 4 - k), x_sem.at[k])
            ring_start(4 - k)

    with jax.named_scope("kv2_wait"):
        landed(kvbuf.at[c, pl.ds(0, RING - 1)], got.at[KV2])
    remote(kvbuf.at[c], kvbuf.at[c], sent.at[KVD], got.at[KVD], (s, other)).start()

    ring_advance(1, (0,))
    with jax.named_scope("pool_halo"):
        landed(p_ext.at[pl.ds(0, 2 * EDGE)], got.at[PH])

    @pl.when(s == 0)
    def _():
        p_ext[pl.ds(0, EDGE), :] = jnp.zeros((EDGE, 2 * HEAD), BF16)

    @pl.when(s == n_sp - 1)
    def _():
        p_ext[pl.ds(EDGE + rows, EDGE), :] = jnp.zeros((EDGE, 2 * HEAD), BF16)

    reach = 1 + (t // 2 > 0) + 2 * (t // 2 > 1) + 4 * (t // 2 > 2)
    span = QB + 2 * EDGE
    apart = (
        lax.broadcasted_iota(jnp.int32, (QB, span), 1)
        - lax.broadcasted_iota(jnp.int32, (QB, span), 0) - EDGE
    )
    band = jnp.where((apart >= -reach) & (apart < reach), 1.0, 0.0).astype(BF16)
    row_id = lax.broadcasted_iota(jnp.int32, (QB, 1), 0)
    scales = jnp.concatenate([scale_v[...], scale_v[...]], axis=1)
    sinks = jnp.broadcast_to(sink_v[...], (1, 2 * HEAD))

    def pool_block(i, carry):
        first = pl.multiple_of(i * QB, QB)
        sums = jnp.dot(band, p_ext[pl.ds(first, span), :], preferred_element_type=F32)
        position = row_id + (s * rows + first)
        counted = (
            jnp.minimum(position + reach, seq_total) - jnp.maximum(position - reach, 0)
        ).astype(F32)
        here = p_ext[pl.ds(pl.multiple_of(EDGE + first, EDGE), QB), :].astype(F32)
        pooled = (sums * (1.0 / counted) - here) * scales
        pool_v[pl.ds(first, QB), :] = swap_halves(pooled).astype(BF16)
        return carry

    with jax.named_scope("pool_mix"):
        lax.fori_loop(0, blocks, pool_block, 0, unroll=2)

    with jax.named_scope("kvd_wait"):
        landed(kvbuf.at[c], got.at[KVD])

    def join_rows(i, carry):
        for j in range(RING):
            at = pl.multiple_of((i * RING + j) * 2 * half_rows, 2 * half_rows)
            wkv[pl.ds(at, half_rows), :] = kvbuf[0, i, j]
            wkv[pl.ds(pl.multiple_of(at + half_rows, half_rows), half_rows), :] = kvbuf[1, j, i]
        return carry

    with jax.named_scope("kv_join"):
        lax.fori_loop(0, RING, join_rows, 0)

    def key_rows(first, count):
        at = pl.ds(pl.multiple_of(first, QB), count)
        value = jnp.dot(nrm[at, :], wkv[...], preferred_element_type=F32)
        kv_ext[pl.ds(pl.multiple_of(WINDOW + first, QB), count), :] = rotated(value, at).astype(BF16)

    ring_advance(1, (3,))
    with jax.named_scope("key_edge"):
        key_rows(0, QB)
        key_rows(rows - QB, QB)
    ring_advance(1, (1,))
    with jax.named_scope("key_rest"):
        key_rows(QB, wide)
    for source, target, device in ((rows, 0, after), (WINDOW, WINDOW + rows, before)):
        remote(
            kv_ext.at[pl.ds(source, WINDOW)], kv_ext.at[pl.ds(target, WINDOW)],
            sent.at[KH], got.at[KH], device,
        ).start()
    far_advance()
    ring_advance(1, (2,))
    with jax.named_scope("key_rest"):
        key_rows(QB + wide, wide)
    with jax.named_scope("key_rest"):
        key_rows(QB + 2 * wide, wide)

    query_at = lax.broadcasted_iota(jnp.int32, (QB, QB), 0)
    key_at = lax.broadcasted_iota(jnp.int32, (QB, QB), 1)

    def across_lanes(column):
        return jnp.broadcast_to(column, (QB, 2 * HEAD))

    def attend(blocks_now):
        window = [kv_ext[pl.ds(i * QB, QB + 2 * WINDOW), :] for i in blocks_now]
        scores = [
            lax.dot_general(
                q_v[pl.ds(i * QB, QB), :], keys, (((1,), (1,)), ((), ())),
                preferred_element_type=F32,
            )
            for i, keys in zip(blocks_now, window)
        ]
        tiles = []
        for i, score in zip(blocks_now, scores):
            low_ok, high_ok = key_at >= query_at, key_at <= query_at
            if i == 0:
                low_ok = low_ok & (s > 0)
            if i == blocks - 1:
                high_ok = high_ok & (s < n_sp - 1)
            tiles.append((
                jnp.where(low_ok, score[:, :QB], NEG_BIG),
                score[:, QB : 2 * QB],
                jnp.where(high_ok, score[:, 2 * QB :], NEG_BIG),
            ))
        highest = [
            jnp.max(jnp.maximum(jnp.maximum(p, q), r), axis=-1, keepdims=True) for p, q, r in tiles
        ]
        highest = [jnp.maximum(across_lanes(top), sinks) for top in highest]
        expo = [[jnp.exp(part - top) for part in three] for three, top in zip(tiles, highest)]
        total = [jnp.sum(p + q + r, axis=-1, keepdims=True) for p, q, r in expo]
        inverse = [
            1.0 / (across_lanes(some) + jnp.exp(sinks - top)) for some, top in zip(total, highest)
        ]
        weights = [
            jnp.concatenate([(part * one).astype(BF16) for part in three], axis=1)
            for three, one in zip(expo, inverse)
        ]
        result = [
            jnp.dot(some, keys, preferred_element_type=F32) for some, keys in zip(weights, window)
        ]
        for i, some in zip(blocks_now, result):
            mix_send[i] = jnp.where(
                lane < HEAD, pool_v[pl.ds(i * QB, QB), :].astype(F32), some
            ).astype(BF16)

    def hand_over(i):
        @pl.when(i != t)
        def _():
            remote(mix_send.at[i], mix_recv.at[t], sent.at[MX], got.at[MX], (s, i)).start()

        @pl.when(i == t)
        def _():
            mix_recv[i] = mix_send[i]

    def attend_pair(i, j):
        with jax.named_scope("attend"):
            attend((i, j))
        hand_over(i)
        hand_over(j)

    attend_pair(1, 2)
    attend_pair(3, 4)
    ring_advance(2, (0,))
    attend_pair(5, 6)
    ring_advance(2, (3,))
    with jax.named_scope("key_halo"):
        landed(kv_ext.at[pl.ds(0, 2 * WINDOW)], got.at[KH])
    attend_pair(0, blocks - 1)
    ring_advance(2, (1,))
    ring_advance(2, (2,))
    far_finish()

    def group_region(owner, group):
        return wbuf.at[owner, pl.ds(0, RING - 2 if group == WD else 1)]

    def cross_wait(group):
        with jax.named_scope("cross_wait"):
            landed(group_region(1 - c, group), got.at[group])

    ring_advance(3, (0, 3, 1, 2))
    cross_wait(WD)

    @pl.when(c == 0)
    def _():
        cross_wait(WL)
        cross_wait(WR)

    left_here(kvbuf.at[c, b, pl.ds(0, RING - 1)], sent.at[KV1])
    with jax.named_scope("mix_wait"):
        landed(mix_recv.at[pl.ds(0, n_tp - 1)], got.at[MX])
    left, right = [], []
    for j in range(n_tp // 2):
        even, odd = mix_recv[2 * j].astype(F32), mix_recv[2 * j + 1].astype(F32)
        left.append(jnp.where(lane < HEAD, swap_halves(even), odd).astype(BF16))
        right.append(jnp.where(lane < HEAD, even, swap_halves(odd)).astype(BF16))
    mixed = jnp.concatenate(left + right, axis=1)

    span_out = RING * width

    def out_block(d):
        i = (z + d) % RING
        parts = []
        for j in range(n_tp // 2):
            parts.append(wbuf[0, i, j].reshape(span_out, QB))
            parts.append(wbuf[1, :, j, i].reshape(span_out, QB))
        cols = pl.ds(pl.multiple_of(i * span_out, span_out), span_out)
        out_v[:, cols] = lax.dot_general(
            mixed, jnp.concatenate(parts, axis=1), (((1,), (1,)), ((), ())),
            preferred_element_type=F32,
        ).astype(BF16)
        store = pltpu.make_async_copy(out_v.at[:, cols], out.at[:, cols], out_sem.at[0])
        store.start()

    with jax.named_scope("out_most"):
        for d in (0, 1, 7, 2, 6, 4):
            out_block(d)

    for d, group in ((3, WL), (5, WR)):
        @pl.when(c == 1)
        def _():
            cross_wait(group)

        with jax.named_scope("out_last"):
            out_block(d)

    with jax.named_scope("send_wait"):
        pltpu.make_async_copy(out_v, out, out_sem.at[0]).wait()
        left_here(kvbuf.at[c, pl.ds(0, RING - 1)], sent.at[KV2])
        left_here(kvbuf.at[c], sent.at[KVD])
        left_here(wbuf.at[c, b, x, pl.ds(0, RING - 1)], sent.at[W1])
        left_here(wbuf.at[c, b, pl.ds(0, 3)], sent.at[W2])
        left_here(group_region(c, WD), sent.at[WD])
        left_here(group_region(c, WL), sent.at[WL])
        left_here(group_region(c, WR), sent.at[WR])
        left_here(part_at(c, b, 0), sent.at[D4])
        left_here(wbuf.at[c, far, pl.ds(0, 3)], sent.at[X4])
        left_here(wbuf.at[c, pl.ds(0, 3)], sent.at[RR])
        left_here(wbuf.at[c, pl.ds(0, 3)], sent.at[RL])
        left_here(p_ext.at[pl.ds(0, 2 * EDGE)], sent.at[PH])
        left_here(kv_ext.at[pl.ds(0, 2 * WINDOW)], sent.at[KH])
        left_here(mix_send.at[pl.ds(0, n_tp - 1)], sent.at[MX])


def body(tokens, norm_gain, w_query, w_key, w_value, w_pool_in, sink_logit, pool_scale, w_out):
    rows, features = tokens.shape
    n_sp, n_tp = lax.axis_size("sp"), lax.axis_size("tp")
    start, row = angle_tables(n_sp, rows)
    dma, vmem = pltpu.SemaphoreType.DMA, pltpu.VMEM
    half = w_key.shape[0] // 2
    width = w_out.shape[1]
    pair = 2 * HEAD
    scratch = [
        vmem((rows, features), BF16),
        vmem((rows, features), BF16),
        vmem((1, features), F32),
        vmem(w_key.shape, BF16),
        vmem(w_value.shape, BF16),
        vmem((1, HEAD), F32),
        vmem((1, 1), F32),
        vmem((8, pair), F32),
        vmem((2, rows, pair), F32),
        vmem((pair, features), BF16),
        vmem((2, RING, RING, half, pair), BF16),
        vmem((features, pair), BF16),
        vmem((2, RING, n_tp // 2, RING, width, w_out.shape[0]), BF16),
        vmem((rows, pair), BF16),
        vmem((rows + 2 * EDGE, pair), BF16),
        vmem((rows, pair), BF16),
        vmem((rows + 2 * WINDOW, pair), BF16),
        vmem((n_tp, QB, pair), BF16),
        vmem((n_tp, QB, pair), BF16),
        vmem((rows // n_tp, width * n_sp), BF16),
        dma((10,)),
        dma((rows // QB,)),
        dma((15,)),
        dma((15,)),
        dma((4,)),
        dma((2, 12)),
        dma((1,)),
    ]
    return pl.pallas_call(
        functools.partial(kernel, rows),
        name="mixer",
        out_shape=jax.ShapeDtypeStruct((rows // n_tp, w_out.shape[1] * n_sp), BF16),
        in_specs=[pl.BlockSpec(memory_space=pl.ANY)] * 11,
        out_specs=pl.BlockSpec(memory_space=pl.ANY),
        scratch_shapes=scratch,
        compiler_params=pltpu.CompilerParams(
            collective_id=0, has_side_effects=True, vmem_limit_bytes=60 * 2**20
        ),
    )(
        tokens, norm_gain[None, :], w_query.T, w_key, w_value, w_pool_in.T, pool_scale[None, :], sink_logit[None, :], w_out.T,
        jnp.asarray(start), jnp.asarray(row),
    )


def solution(mesh):
    in_specs = (
        P("sp", None),
        P(),
        P(None, "tp"),
        P("sp", None),
        P("sp", None),
        P(None, "tp"),
        P("tp"),
        P("tp"),
        P("tp", "sp"),
    )
    out_specs = P(("sp", "tp"), None)
    return jax.shard_map(body, mesh=mesh, in_specs=in_specs, out_specs=out_specs, check_vma=False)
```
